32 devices in a mesh: sp: 8 (over z, y), tp: 4 (over x, core).
Axes of the slice: x: 2, y: 2, z: 4, core: 2. Of those that a mesh axis runs over, the one named last changes fastest.
Arguments:
- latent: bfloat16 [4096, 2048], P(('sp', 'tp')), may hold values from -6 to 6
- context: bfloat16 [512, 2048], P('sp'), may hold values from -6 to 6
- condition: float32 [2048], replicated, may hold values from -6 to 6
- context_condition: float32 [2048], replicated, may hold values from -6 to 6
- norm_gain: float32 [2048], replicated, may hold values from 0.1 to 1.9
- shift_weight: bfloat16 [2048, 2048], P('sp', 'tp'), may hold values from -0.21875 to 0.21875
- scale_weight: bfloat16 [2048, 2048], P('sp', 'tp'), may hold values from -0.21875 to 0.21875
- gate_weight: bfloat16 [2048, 2048], P('sp', 'tp'), may hold values from -0.21875 to 0.21875
- query_weight: bfloat16 [2048, 1024], P(None, 'tp'), may hold values from -1 to 1
- key_weight: bfloat16 [2048, 512], P(None, 'tp'), may hold values from -1 to 1
- value_weight: bfloat16 [2048, 512], P(None, 'tp'), may hold values from -0.125 to 0.125
- query_gain: float32 [64], replicated, may hold values from 0.1 to 7.8
- key_gain: float32 [64], replicated, may hold values from 0.1 to 7.8
- output_weight: bfloat16 [1024, 2048], replicated, may hold values from -1 to 1
Outputs:
- updated: bfloat16 [4096, 2048], P(('sp', 'tp'))
The draws below stay inside these ranges and needn't reach their ends.
All inputs are finite; a program needn't handle non-finite values.
Results may differ from the reference program's by a relative error of at most 0.012.
The reference program's roundings to bfloat16 on the way count: a program that leaves them out, or rounds other values in their place, can miss the bound.
Values may be sent and summed in bfloat16 or wider, within the bound.
A program may use at most 64 MiB of HBM per device.

```python
import math
import jax
import jax.numpy as jnp
from jax import lax

D = 2048
HQ = 16
KVH = 8
CHANNEL_SPAN = 64
GRID_W = 64
PREFIX_ITEMS = 512
HIDDEN_ITEMS = 4096


def query_base(key):
    return jax.random.truncated_normal(jax.random.fold_in(key, 101), -6.0, 6.0, (D, HQ * CHANNEL_SPAN), jnp.float32) * D ** (-0.5)


def draw_query_weight(key, part):
    return query_base(key).astype(jnp.bfloat16)


def draw_key_weight(key, part):
    fresh = jax.random.truncated_normal(jax.random.fold_in(key, 102), -6.0, 6.0, (D, KVH * CHANNEL_SPAN), jnp.float32) * D ** (-0.5)
    return fresh.astype(jnp.bfloat16)


def gain_draw(key, salt):
    return 3.0 * (1.0 + 0.18 * jax.random.truncated_normal(jax.random.fold_in(key, salt), -5.0, 5.0, (CHANNEL_SPAN,), jnp.float32))


def draw_query_gain(key, part):
    return gain_draw(key, 103)


def draw_key_gain(key, part):
    return gain_draw(key, 104)


def draw_output_weight(key, part):
    base = jax.random.truncated_normal(jax.random.fold_in(key, 105), -6.0, 6.0, (HQ * CHANNEL_SPAN, D), jnp.float32)
    return (base * (HQ * CHANNEL_SPAN) ** (-0.5)).astype(jnp.bfloat16)


def steps_of(own_key, dims, pieces, low, largest):
    loudness = 1.0
    for dim, parts in pieces:
        draws = jax.random.uniform(jax.random.fold_in(jax.random.fold_in(own_key, 6), dim), (parts,), jnp.float32, low / len(pieces), largest / len(pieces))
        loudness = loudness * jnp.repeat(jnp.exp(draws), dims[dim] // parts).reshape((-1,) + (1,) * (len(dims) - 1 - dim))
    return loudness


def scatter_about(key, extent, deviation, most, shards=(), kind=jnp.bfloat16):
    entries = deviation * jax.random.normal(key, extent, jnp.float32)
    if shards:
        entries = entries * steps_of(key, extent, shards, -0.22, 0.18)
    return jnp.clip(entries, -most, most).astype(kind)


def setup_inputs(seed: int = 0) -> dict:
    keys = jax.random.split(jax.random.key(seed), 15)
    latent = scatter_about(keys[0], (HIDDEN_ITEMS, D), 1.0, 6.0, ((0, 32),))
    context = scatter_about(keys[1], (PREFIX_ITEMS, D), 1.0, 6.0, ((0, 8),))
    condition = scatter_about(keys[2], (D,), 1.0, 6.0, (), jnp.float32)
    context_condition = scatter_about(keys[3], (D,), 1.0, 6.0, (), jnp.float32)
    norm_gain = jnp.clip(1.0 + 0.18 * jax.random.normal(keys[4], (D,), jnp.float32), 0.1, 1.9)
    shift_weight = scatter_about(keys[5], (D, D), (D // 3) ** -0.5, 0.21875, ((0, 8), (1, 4)))
    scale_weight = scatter_about(keys[6], (D, D), (D // 3) ** -0.5, 0.21875, ((0, 8), (1, 4)))
    gate_weight = scatter_about(keys[7], (D, D), (D // 3) ** -0.5, 0.21875, ((0, 8), (1, 4)))
    query_weight = draw_query_weight(jax.random.fold_in(keys[14], 71), 0)
    key_weight = draw_key_weight(jax.random.fold_in(keys[14], 71), 0)
    value_weight = scatter_about(keys[10], (D, KVH * CHANNEL_SPAN), D ** -0.5, 0.125, ((1, 4),))
    query_gain = draw_query_gain(jax.random.fold_in(keys[14], 71), 0)
    key_gain = draw_key_gain(jax.random.fold_in(keys[14], 71), 0)
    output_weight = draw_output_weight(jax.random.fold_in(keys[14], 71), 0)
    return {"latent": latent, "context": context, "condition": condition, "context_condition": context_condition, "norm_gain": norm_gain, "shift_weight": shift_weight, "scale_weight": scale_weight, "gate_weight": gate_weight, "query_weight": query_weight, "key_weight": key_weight, "value_weight": value_weight, "query_gain": query_gain, "key_gain": key_gain, "output_weight": output_weight}


epsilon = 1e-06
rope_base = 10000.0

def modulate(tok_rows, norm_gain, shift_row, scale_row):
    wide = tok_rows.astype(jnp.float32)
    normed = wide * lax.rsqrt(lax.optimization_barrier(jnp.mean(wide * wide, axis=-1, keepdims=True)) + epsilon)
    return (normed * norm_gain * (1.0 + scale_row) + shift_row).astype(jnp.bfloat16)

def headnorm(raw, gain, heads):
    field = raw.reshape(raw.shape[0], heads, -1)
    return field * lax.rsqrt(lax.optimization_barrier(jnp.mean(field * field, axis=-1, keepdims=True)) + epsilon) * gain

def rotate(field, places):
    count = field.shape[0]
    heads = field.shape[1]
    quarter = field.shape[2] // 4
    grid_row = (places // GRID_W).astype(jnp.float32)
    grid_col = (places % GRID_W).astype(jnp.float32)
    inverse = rope_base ** (-jnp.arange(quarter, dtype=jnp.float32) / quarter)
    angles = jnp.stack([grid_row[:, None] * inverse, grid_col[:, None] * inverse], axis=1)[:, None]
    cosine = jnp.cos(angles)
    sine = jnp.sin(angles)
    matcher_content_couples = field.reshape(count, heads, 2, 2, quarter)
    first = matcher_content_couples[:, :, :, 0]
    second = matcher_content_couples[:, :, :, 1]
    turned = jnp.stack([first * cosine - second * sine, second * cosine + first * sine], axis=3)
    return turned.reshape(count, heads, 4 * quarter)

def reference(latent, context, condition, context_condition, norm_gain, shift_weight, scale_weight, gate_weight, query_weight, key_weight, value_weight, query_gain, key_gain, output_weight):
    activated = jax.nn.silu(jnp.stack([condition, context_condition])).astype(jnp.bfloat16)
    shifts = jnp.dot(activated, shift_weight, preferred_element_type=jnp.float32)
    scales = jnp.dot(activated, scale_weight, preferred_element_type=jnp.float32)
    gates = jnp.dot(activated, gate_weight, preferred_element_type=jnp.float32)
    hidden = modulate(latent, norm_gain, shifts[0], scales[0])
    context_hidden = modulate(context, norm_gain, shifts[1], scales[1])
    places = jnp.arange(HIDDEN_ITEMS, dtype=jnp.int32)
    probe_entries = rotate(headnorm(jnp.dot(hidden, query_weight, preferred_element_type=jnp.float32), query_gain, HQ), places).astype(jnp.bfloat16)
    latent_keys = rotate(headnorm(jnp.dot(hidden, key_weight, preferred_element_type=jnp.float32), key_gain, KVH), places).astype(jnp.bfloat16)
    latent_values = jnp.dot(hidden, value_weight, preferred_element_type=jnp.float32).astype(jnp.bfloat16).reshape(HIDDEN_ITEMS, KVH, CHANNEL_SPAN)
    context_keys = headnorm(jnp.dot(context_hidden, key_weight, preferred_element_type=jnp.float32), key_gain, KVH).astype(jnp.bfloat16)
    context_values = jnp.dot(context_hidden, value_weight, preferred_element_type=jnp.float32).astype(jnp.bfloat16).reshape(PREFIX_ITEMS, KVH, CHANNEL_SPAN)
    matcher_pieces = jnp.concatenate([context_keys, latent_keys], axis=0).astype(jnp.float32)
    value_rows = jnp.concatenate([context_values, latent_values], axis=0).astype(jnp.float32)
    prefix_mapped = math.log(HIDDEN_ITEMS / (2.0 * PREFIX_ITEMS))
    similarity_offset = jnp.concatenate([jnp.full((PREFIX_ITEMS,), prefix_mapped, jnp.float32), jnp.zeros((HIDDEN_ITEMS,), jnp.float32)])
    group_size = HQ // KVH
    group_extent = math.gcd(HIDDEN_ITEMS, 256)
    grouped = probe_entries.reshape(HIDDEN_ITEMS // group_extent, group_extent, KVH, group_size, CHANNEL_SPAN)

    def one_block(probe_segment):
        similarity_matrix = jnp.einsum('dmvk,hmk->dmvh', probe_segment.astype(jnp.float32), matcher_pieces) * CHANNEL_SPAN ** (-0.5) + similarity_offset
        row_peak = lax.optimization_barrier(jnp.max(similarity_matrix, axis=-1, keepdims=True))
        shares = jnp.exp(similarity_matrix - row_peak)
        row_total = lax.optimization_barrier(jnp.sum(shares, axis=-1))
        rounded = lax.optimization_barrier(shares.astype(jnp.bfloat16)).astype(jnp.float32)
        weighted = jnp.einsum('qkgn,nkd->qkgd', rounded, value_rows)
        return (weighted / row_total[..., None]).astype(jnp.bfloat16)
    attended = lax.map(one_block, grouped).reshape(HIDDEN_ITEMS, HQ * CHANNEL_SPAN)
    projected = jnp.dot(attended, output_weight, preferred_element_type=jnp.float32)
    return (latent.astype(jnp.float32) + gates[0] * projected).astype(jnp.bfloat16)
```

```python
import functools
import math

import jax
import jax.numpy as jnp
from jax import lax
from jax.experimental import pallas as pl
from jax.experimental.pallas import tpu as pltpu
from jax.sharding import PartitionSpec as P

SPAN = 64
GRID_W = 64
QUARTER = SPAN // 4
LAG = 3
PIECES = 2
LOG2E = 1.4426950408889634
MESH = pl.DeviceIdType.MESH
VMEM = pl.BlockSpec(memory_space=pltpu.VMEM)
ANY = pl.BlockSpec(memory_space=pl.ANY)
F32 = jnp.float32
BF16 = jnp.bfloat16

epsilon = 1e-06
rope_base = 10000.0


def kernel(
    n_sp, n_tp, lows, offset,
    latent_hbm, context_hbm, cond, ctx_cond, norm_gain, w_shift_hbm, w_scale_hbm, w_gate_hbm,
    w_q_hbm, w_k_hbm, w_v_hbm, q_gain, k_gain, w_out_hbm,
    out,
    lat, context, w_mod, w_all, w_side, w_out, part, parts, mods, coef, hidden,
    table, gain_q, gain_k, q_send, kv_send, ctx_send, ctx_all, q_all, kv_all, k_nat,
    peak, total, acc, attended, received,
    load, lat_send, lat_fwd, lat_recv, sp_send, sp_recv, tp_send, tp_recv,
    q_ssem, q_rsem, z_send, y_send, f_send, kv_recv,
    cz_send, cy_send, cf_send, c_recv, at_send, at_recv,
):
    sp, tp = lax.axis_index("sp"), lax.axis_index("tp")
    chips = n_tp // 2
    highs = n_sp // lows
    low, high = lax.rem(sp, lows), sp // lows
    x, core = tp // 2, lax.rem(tp, 2)
    twin = tp + 1 - 2 * core
    width = lat.shape[1]
    own_rows = width // 2
    model = lat.shape[2]
    tok = chips * width
    ctx_rows = context.shape[0]
    groups = kv_send.shape[1]
    heads = q_send.shape[2]
    q_width = groups * heads * SPAN
    kv_width = groups * SPAN
    row_slab, columns = w_mod.shape[1], w_mod.shape[2]
    g = lax.rem(high, groups)
    base = high - g
    ctx_slots = n_sp * ctx_rows // width
    ctx_first = chips * n_sp

    def dev(z, y):
        return z * lows + y

    def remote(src, dst, ssem, rsem, peer):
        return pltpu.make_async_remote_copy(
            src_ref=src, dst_ref=dst, send_sem=ssem, recv_sem=rsem,
            device_id=peer, device_id_type=MESH,
        )

    def own_part(ref, chip, half):
        return ref.at[chip, pl.ds(pl.multiple_of(half * own_rows, own_rows), own_rows), :]

    pairs = [
        (latent_hbm, own_part(lat, x, core)),
        (w_shift_hbm, w_mod.at[0]), (w_scale_hbm, w_mod.at[1]), (w_gate_hbm, w_mod.at[2]),
        (context_hbm, context), (w_q_hbm, w_all.at[:, 0:q_width]),
    ]
    if kv_width % 128 == 0:
        pairs += [
            (w_k_hbm, w_all.at[:, q_width : q_width + kv_width]),
            (w_v_hbm, w_all.at[:, q_width + kv_width :]),
        ]
    else:
        pairs += [(w_k_hbm, w_side.at[0]), (w_v_hbm, w_side.at[1])]
    pairs.append((w_out_hbm, w_out))
    loads = [pltpu.make_async_copy(s, d, load.at[i]) for i, (s, d) in enumerate(pairs)]
    for c in loads:
        c.start()

    barrier = pltpu.get_barrier_semaphore()
    peers = [(lax.rem(sp + d, n_sp), tp) for d in range(1, n_sp)]
    peers += [(sp, lax.rem(tp + d, n_tp)) for d in range(1, n_tp)]
    for r in range(1, groups):
        mate = dev(base + lax.rem(g + r, groups), low)
        peers += [(mate, lax.rem(tp + d, n_tp)) for d in range(1, n_tp)]
    for p in peers:
        pl.semaphore_signal(barrier, inc=1, device_id=p, device_id_type=MESH)
    pl.semaphore_wait(barrier, len(peers))

    step = own_rows // PIECES

    def rows_of(tile, piece):
        chip, half = tile // 2, lax.rem(tile, 2)
        start = pl.multiple_of(half * own_rows + piece * step, step)
        return lat.at[chip, pl.ds(start, step), :]

    def row_copy(tile, piece, ssem, peer):
        return remote(
            rows_of(tile, piece), rows_of(tile, piece), ssem, lat_recv.at[tile, piece], (sp, peer)
        )

    lat_sends = []

    def send_piece(piece):
        for d in range(1, chips):
            c = row_copy(tp, piece, lat_send.at[d, piece], lax.rem(tp + 2 * d, n_tp))
            c.start()
            lat_sends.append(c)

    loads[0].wait()
    send_piece(0)
    for piece in range(PIECES):
        c = row_copy(tp, piece, lat_send.at[0, piece], twin)
        c.start()
        lat_sends.append(c)

    def slab(ref):
        if row_slab % 128 == 0:
            return ref[:, pl.ds(pl.multiple_of(sp * row_slab, 128), row_slab)]
        per = 128 // row_slab
        window = ref[:, pl.ds(pl.multiple_of(sp // per * 128, 128), 128)]
        pick = lax.rem(sp, per)
        result = window
        for k in range(1, per):
            result = jnp.where(pick == k, pltpu.roll(window, 128 - k * row_slab, 1), result)
        return result[:, :row_slab]

    v = jnp.concatenate([slab(cond), slab(ctx_cond)], axis=0)
    act = (v / (1.0 + jnp.exp(-v))).astype(BF16)
    part[...] = jnp.zeros_like(part)
    for i in range(3):
        loads[1 + i].wait()
        part[2 * i : 2 * i + 2, :] = jnp.dot(act, w_mod[i], preferred_element_type=F32)
    sp_copies = []
    for d in range(1, n_sp):
        c = remote(
            part, parts.at[sp], sp_send.at[d - 1], sp_recv.at[d - 1], (lax.rem(sp + d, n_sp), tp)
        )
        c.start()
        sp_copies.append(c)
    parts[sp] = part[...]

    for d in range(chips):
        chip = lax.rem(x - d + chips, chips)
        place = sp * tok + chip * width + lax.broadcasted_iota(jnp.int32, (QUARTER, width), 1)
        turn = lax.broadcasted_iota(jnp.int32, (QUARTER, width), 0).astype(F32)
        freq = jnp.exp(turn * (-math.log(rope_base) / QUARTER))
        by_row = (place // GRID_W).astype(F32) * freq
        by_col = (place % GRID_W).astype(F32) * freq
        table[d, 0:QUARTER, :] = jnp.cos(by_row)
        table[d, QUARTER : 2 * QUARTER, :] = jnp.sin(by_row)
        table[d, 2 * QUARTER : 3 * QUARTER, :] = jnp.cos(by_col)
        table[d, 3 * QUARTER :, :] = jnp.sin(by_col)
    k_pair = jnp.concatenate([k_gain[...], k_gain[...]], axis=1)
    for ref, dst in ((q_gain, gain_q), (k_gain, gain_k)):
        row = jnp.concatenate([ref[...], ref[...]], axis=1)
        square = jnp.transpose(jnp.broadcast_to(row, (128, 128)))[0:SPAN, :]
        for c in range(0, width, 128):
            dst[:, c : c + 128] = square
    peak[...] = jnp.full_like(peak, -1e30)
    total[...] = jnp.zeros_like(total)
    acc[...] = jnp.zeros_like(acc)
    q_all[:, :, SPAN:, :] = jnp.zeros((q_all.shape[0], heads, SPAN, width), BF16)

    for c in sp_copies:
        c.wait()
    summed = parts[0]
    for j in range(1, n_sp):
        summed = summed + parts[j]
    part[...] = summed
    mods[tp] = summed
    tp_copies = []
    for d in range(1, n_tp):
        c = remote(
            part, mods.at[tp], tp_send.at[d - 1], tp_recv.at[d - 1], (sp, lax.rem(tp + d, n_tp))
        )
        c.start()
        tp_copies.append(c)
    for piece in range(1, PIECES):
        send_piece(piece)
    for c in loads[4:-1]:
        c.wait()
    if kv_width % 128 != 0:
        w_all[:, q_width:] = jnp.concatenate([w_side[0], w_side[1]], axis=1)
    for piece in range(PIECES):
        row_copy(twin, piece, lat_send.at[0, 0], twin).wait_recv()
    for c in tp_copies:
        c.wait()
    for t in range(n_tp):
        cols = slice(t * columns, (t + 1) * columns)
        for row in range(2):
            coef[row : row + 1, cols] = norm_gain[:, cols] * (1.0 + mods[t, 2 + row : 3 + row, :])
            coef[2 + row : 3 + row, cols] = mods[t, row : row + 1, :]

    block = 16

    def modulate(read, rows, row):
        def body(i, carry):
            r = pl.ds(pl.multiple_of(i * block, block), block)
            w = read(r).astype(F32)
            inv = lax.rsqrt(jnp.sum(w * w, axis=-1, keepdims=True) / model + epsilon)
            y = w * inv * coef[row : row + 1, :] + coef[2 + row : 3 + row, :]
            hidden[r, :] = y.astype(BF16)
            return carry

        lax.fori_loop(0, rows // block, body, 0, unroll=min(4, rows // block))

    modulate(lambda r: context[r, :], ctx_rows, 1)
    raw = jnp.dot(hidden[0:ctx_rows, :], w_all[:, q_width:], preferred_element_type=F32)
    if groups == 2:
        k, val = raw[:, :kv_width], raw[:, kv_width:]
        lane = lax.broadcasted_iota(jnp.int32, k.shape, 1)
        first = lane < SPAN
        sq = k * k
        s0 = jnp.sum(jnp.where(first, sq, 0.0), axis=-1, keepdims=True)
        s1 = jnp.sum(jnp.where(first, 0.0, sq), axis=-1, keepdims=True)
        scale = jnp.where(
            first, lax.rsqrt(s0 / SPAN + epsilon), lax.rsqrt(s1 / SPAN + epsilon)
        )
        k = k * scale * k_pair
        ctx_send[0] = jnp.where(first, k, pltpu.roll(val, SPAN, 1)).astype(BF16)
        ctx_send[1] = jnp.where(first, pltpu.roll(k, SPAN, 1), val).astype(BF16)
    else:
        lane = lax.broadcasted_iota(jnp.int32, raw.shape, 1)
        first = lane < SPAN
        s0 = jnp.sum(jnp.where(first, raw * raw, 0.0), axis=-1, keepdims=True)
        k = raw * lax.rsqrt(s0 / SPAN + epsilon) * k_pair
        ctx_send[0] = jnp.where(first, k, raw).astype(BF16)
    far = [d for d in range(2, highs)] if highs > 2 else []
    z_order = far[:1] + [1] + far[1:] if highs > 1 else []
    tail_sends = []

    def ctx_copy(head, src, ssem, z, y):
        return remote(ctx_send.at[head], ctx_all.at[src], ssem, c_recv.at[src], (dev(z, y), tp))

    def finish(raw_head, gain, d):
        inv = lax.rsqrt(jnp.sum(raw_head * raw_head, axis=0, keepdims=True) / SPAN + epsilon)
        y = raw_head * inv * gain[...]
        a1, b1 = y[0:QUARTER], y[QUARTER : 2 * QUARTER]
        a2, b2 = y[2 * QUARTER : 3 * QUARTER], y[3 * QUARTER :]
        cr, sr = table[d, 0:QUARTER, :], table[d, QUARTER : 2 * QUARTER, :]
        cc, sc = table[d, 2 * QUARTER : 3 * QUARTER, :], table[d, 3 * QUARTER :, :]
        return jnp.concatenate(
            [a1 * cr - b1 * sr, b1 * cr + a1 * sr, a2 * cc - b2 * sc, b2 * cc + a2 * sc], axis=0
        )

    def q_copy(d, group, ssem, z):
        return remote(
            q_send.at[d, group], q_all.at[d * groups + g, :, 0:SPAN, :], ssem,
            q_rsem.at[d, g], (dev(z, low), tp),
        )

    def q_arrive(d, r):
        other = lax.rem(g + r, groups)
        remote(
            q_send.at[d, other], q_all.at[d * groups + other, :, 0:SPAN, :], q_ssem.at[d, 0],
            q_rsem.at[d, other], (dev(base + other, low), tp),
        ).wait_recv()

    def kv_copy(src_ref, d, src, ssem, z, y):
        return remote(
            src_ref, kv_all.at[d * n_sp + src], ssem, kv_recv.at[d, src], (dev(z, y), tp)
        )

    def project(d):
        chip = lax.rem(x - d + chips, chips)
        modulate(lambda r: lat[chip, r, :], width, 0)
        flat = jnp.dot(hidden[...], w_all[...], preferred_element_type=F32)
        up = jnp.transpose(flat)
        for j in range(groups):
            for h in range(heads):
                r = (j * heads + h) * SPAN
                y = finish(up[r : r + SPAN], gain_q, d)
                q_send[d, j, h] = (y * SPAN ** (-0.5)).astype(BF16)
            r = q_width + j * SPAN
            kv_send[d, j, 0:SPAN, :] = finish(up[r : r + SPAN], gain_k, d).astype(BF16)
            r = q_width + kv_width + j * SPAN
            kv_send[d, j, SPAN:, :] = up[r : r + SPAN].astype(BF16)
        for r in range(1, groups):
            other = lax.rem(g + r, groups)
            c = q_copy(d, other, q_ssem.at[d, r - 1], base + other)
            c.start()
            tail_sends.append(c)
        for n, dz in enumerate(z_order):
            z = lax.rem(high + dz, highs)
            head = lax.rem(z, groups)
            if d == 0:
                c = ctx_copy(head, sp, cz_send.at[dz - 1], z, low)
                c.start()
                tail_sends.append(c)
            c = kv_copy(kv_send.at[d, head], d, sp, z_send.at[d, dz - 1], z, low)
            c.start()
            tail_sends.append(c)
        for dl in range(1, lows):
            y = lax.rem(low + dl, lows)
            if d == 0:
                c = ctx_copy(g, sp, cy_send.at[dl - 1], high, y)
                c.start()
                tail_sends.append(c)
            c = kv_copy(kv_send.at[d, g], d, sp, y_send.at[d, dl - 1], high, y)
            c.start()
            tail_sends.append(c)
        q_all[d * groups + g, :, 0:SPAN, :] = q_send[d, g]
        kv_all[d * n_sp + sp] = kv_send[d, g]
        k_nat[d * n_sp + sp] = jnp.transpose(kv_send[d, g])
        if d == 0:
            ctx_all[sp] = ctx_send[g]

    def column(d, dz):
        src = dev(lax.rem(high - dz + highs, highs), low)
        slot = d * n_sp + src
        kv_copy(kv_all.at[slot], d, src, z_send.at[0, 0], high, low).wait_recv()
        for dl in range(1, lows):
            y = lax.rem(low + dl, lows)
            c = kv_copy(kv_all.at[slot], d, src, f_send.at[d, dz - 1, dl - 1], high, y)
            c.start()
            tail_sends.append(c)
        k_nat[slot] = jnp.transpose(kv_all[slot])
        if d == 0:
            ctx_copy(0, src, cz_send.at[0], high, low).wait_recv()
            for dl in range(1, lows):
                y = lax.rem(low + dl, lows)
                c = remote(
                    ctx_all.at[src], ctx_all.at[src], cf_send.at[dz - 1, dl - 1],
                    c_recv.at[src], (dev(high, y), tp),
                )
                c.start()
                tail_sends.append(c)

    def side(d, dz, dl):
        src = dev(lax.rem(high - dz + highs, highs), lax.rem(low - dl + lows, lows))
        slot = d * n_sp + src
        kv_copy(kv_all.at[slot], d, src, z_send.at[0, 0], high, low).wait_recv()
        k_nat[slot] = jnp.transpose(kv_all[slot])
        return slot

    def own_slot(d, dz):
        return d * n_sp + dev(lax.rem(high - dz + highs, highs), low)

    def attend(items):
        items = [(s, t, h, b) for s, t, b in items for h in range(heads)]
        n = len(items)
        scores = {}

        def score(i):
            s, t, h, b = items[i]
            r = jnp.dot(k_nat[s], q_all[t, h], preferred_element_type=F32)
            scores[i] = r + b if b else r

        for i in range(min(LAG, n)):
            score(i)
        for i in range(n):
            if i + LAG < n:
                score(i + LAG)
            slot, t, h, _ = items[i]
            s = scores.pop(i)
            old = peak[t, h, 0:1, :]
            top = jnp.maximum(jnp.max(s, axis=0, keepdims=True), old)
            shrink = jnp.exp2((old - top) * LOG2E)
            e = jnp.exp2((s - top) * LOG2E)
            total[t, h] = total[t, h] * shrink + jnp.sum(
                e.reshape(width // 8, 8, width), axis=0
            )
            peak[t, h] = jnp.broadcast_to(top, (8, width))
            w = jnp.dot(kv_all[slot, SPAN:, :], e.astype(BF16), preferred_element_type=F32)
            acc[t, h] = acc[t, h] * shrink + w

    def tiles(d):
        return range(d * groups, (d + 1) * groups)

    def attend_range(first, count, tile_list, shift):
        per = max(1, 8 // len(tile_list))
        per = math.gcd(per, count)

        def body(i, carry):
            attend(
                [(first + i * per + u, t, shift) for u in range(per) for t in tile_list]
            )
            return carry

        if count == per:
            body(0, 0)
        else:
            lax.fori_loop(0, count // per, body, 0)

    def fetch(d):
        chip = lax.rem(x - d + chips, chips)
        near, back = 2 * chip + core, 2 * chip + 1 - core
        for piece in range(PIECES):
            row_copy(near, piece, lat_send.at[0, 0], twin).wait_recv()
            c = row_copy(near, piece, lat_fwd.at[d - 1, piece], twin)
            c.start()
            tail_sends.append(c)
        return back

    def fetch_rest(back):
        for piece in range(PIECES):
            row_copy(back, piece, lat_send.at[0, 0], twin).wait_recv()

    project(0)
    pending = list(z_order)
    for d in range(chips):
        mine = [t for t in tiles(d)]
        so_far = [t for t in range((d + 1) * groups)]
        done = []
        for r in range(1, groups):
            q_arrive(d, r)
        if d > 0:
            segments = [(k * n_sp, n_sp) for k in range(d)]
            if len(segments) < len(pending):
                segments = [(k * n_sp // 2, n_sp // 2) for k in range(2 * d)]
            for first, count in segments:
                attend_range(first, count, mine, 0.0)
                if pending:
                    dz = pending.pop(0)
                    column(d, dz)
                    done.append(dz)
        if d == chips - 1:
            for dz in pending:
                column(d, dz)
                done.append(dz)
            pending = []
        else:
            attend([(own_slot(d, 0), t, 0.0) for t in so_far])
            dz = pending.pop(0)
            column(d, dz)
            attend([(own_slot(d, dz), t, 0.0) for t in so_far])
            back = fetch(d + 1)
            if pending:
                extra = pending.pop(0)
                column(d, extra)
                done.append(extra)
            fetch_rest(back)
            project(d + 1)
            for dz in pending:
                column(d, dz)
                done.append(dz)
            pending = list(z_order)
        if d == chips - 1:
            done = [0] + done
        if d == 0:
            for dl in range(1, lows):
                for dz in range(highs):
                    src = dev(
                        lax.rem(high - dz + highs, highs), lax.rem(low - dl + lows, lows)
                    )
                    ctx_copy(0, src, cz_send.at[0], high, low).wait_recv()
            for c in range(ctx_slots):
                per = width // ctx_rows
                piece = ctx_all[c * per : (c + 1) * per].reshape(width, 2 * SPAN)
                k_nat[ctx_first + c] = piece
                kv_all[ctx_first + c] = jnp.transpose(piece)
        for i in range(0, len(done), 2):
            attend([(own_slot(d, dz), t, 0.0) for dz in done[i : i + 2] for t in so_far])
        attend_range(ctx_first, ctx_slots, mine, offset)
        for dl in range(1, lows):
            order = [0] + list(z_order)
            for i in range(0, len(order), 2):
                slots = [side(d, dz, dl) for dz in order[i : i + 2]]
                attend([(s, t, 0.0) for s in slots for t in so_far])

    copies = []
    for d in range(chips):
        chip = lax.rem(x - d + chips, chips)
        for r in reversed(range(groups)):
            j = lax.rem(g + r, groups)
            t = d * groups + j
            rows = []
            for h in range(heads):
                inv = 1.0 / jnp.sum(total[t, h], axis=0, keepdims=True)
                rows.append(acc[t, h] * inv)
            attended[d, r] = jnp.transpose(jnp.concatenate(rows, axis=0)).astype(BF16)
            for rc in range(2):
                half = lax.rem(core + rc, 2)
                src = attended.at[
                    d, r, pl.ds(pl.multiple_of(half * own_rows, own_rows), own_rows), :
                ]
                if d == 0 and r == 0 and rc == 0:
                    received[tp * groups + g] = src[...]
                else:
                    c = remote(
                        src, received.at[tp * groups + g], at_send.at[d, r, rc],
                        at_recv.at[tp * groups + g],
                        (dev(base + j, low), 2 * chip + half),
                    )
                    c.start()
                    copies.append(c)
    loads[-1].wait()
    for rt in range(n_tp):
        for r in range(groups):
            if rt == 0 and r == 0:
                continue
            who = lax.rem(tp + rt, n_tp) * groups + lax.rem(g + r, groups)
            remote(
                received.at[who], received.at[who], at_send.at[0, 0, 1], at_recv.at[who],
                (sp, twin),
            ).wait_recv()
    rows = jnp.concatenate([received[s] for s in range(n_tp * groups)], axis=1)
    own = pl.ds(pl.multiple_of(core * own_rows, own_rows), own_rows)
    for t in range(n_tp):
        cols = slice(t * columns, (t + 1) * columns)
        branch = jnp.dot(rows, w_out[:, cols], preferred_element_type=F32)
        out[:, cols] = (lat[x, own, cols].astype(F32) + mods[t, 4:5, :] * branch).astype(BF16)
    for c in lat_sends + tail_sends + copies:
        c.wait_send()


def on_device(
    latent, context, condition, context_condition, norm_gain, shift_weight, scale_weight,
    gate_weight, query_weight, key_weight, value_weight, query_gain, key_gain, output_weight,
):
    n_sp, n_tp = lax.axis_size("sp"), lax.axis_size("tp")
    row_slab, columns = shift_weight.shape
    own_rows, model = latent.shape
    ctx_rows = context.shape[0]
    tok = own_rows * n_tp
    q_width, kv_width = query_weight.shape[1], key_weight.shape[1]
    groups = kv_width // SPAN
    heads = q_width // SPAN // groups
    chips = n_tp // 2
    width = 2 * own_rows
    lows = 2 ** (int(math.log2(n_sp)) // 2)
    highs = n_sp // lows
    slots = chips * n_sp + n_sp * ctx_rows // width
    n_tiles = chips * groups
    offset = math.log(tok / (2.0 * ctx_rows))
    dma = pltpu.SemaphoreType.DMA
    return pl.pallas_call(
        functools.partial(kernel, n_sp, n_tp, lows, offset),
        out_shape=jax.ShapeDtypeStruct(latent.shape, BF16),
        in_specs=[ANY] * 2 + [VMEM] * 3 + [ANY] * 6 + [VMEM] * 2 + [ANY],
        out_specs=VMEM,
        scratch_shapes=[
            pltpu.VMEM((chips, width, model), BF16),
            pltpu.VMEM(context.shape, BF16),
            pltpu.VMEM((3, row_slab, columns), BF16),
            pltpu.VMEM((model, q_width + 2 * kv_width), BF16),
            pltpu.VMEM((2,) + (key_weight.shape if kv_width % 128 else (16, 128)), BF16),
            pltpu.VMEM(output_weight.shape, BF16),
            pltpu.VMEM((8, columns), F32),
            pltpu.VMEM((n_sp, 8, columns), F32),
            pltpu.VMEM((n_tp, 8, columns), F32),
            pltpu.VMEM((8, model), F32),
            pltpu.VMEM((width, model), BF16),
            pltpu.VMEM((chips, SPAN, width), F32),
            pltpu.VMEM((SPAN, width), F32),
            pltpu.VMEM((SPAN, width), F32),
            pltpu.VMEM((chips, groups, heads, SPAN, width), BF16),
            pltpu.VMEM((chips, groups, 2 * SPAN, width), BF16),
            pltpu.VMEM((groups, ctx_rows, 2 * SPAN), BF16),
            pltpu.VMEM((n_sp, ctx_rows, 2 * SPAN), BF16),
            pltpu.VMEM((n_tiles, heads, 2 * SPAN, width), BF16),
            pltpu.VMEM((slots, 2 * SPAN, width), BF16),
            pltpu.VMEM((slots, width, 2 * SPAN), BF16),
            pltpu.VMEM((n_tiles, heads, 8, width), F32),
            pltpu.VMEM((n_tiles, heads, 8, width), F32),
            pltpu.VMEM((n_tiles, heads, SPAN, width), F32),
            pltpu.VMEM((chips, groups, width, 2 * SPAN), BF16),
            pltpu.VMEM((n_tp * groups, own_rows, 2 * SPAN), BF16),
            dma((9,)), dma((chips, PIECES)), dma((max(chips - 1, 1), PIECES)), dma((n_tp, PIECES)),
            dma((n_sp - 1,)), dma((n_sp - 1,)), dma((n_tp - 1,)), dma((n_tp - 1,)),
            dma((chips, max(groups - 1, 1))), dma((chips, groups)),
            dma((chips, highs - 1)), dma((chips, lows - 1)),
            dma((chips, highs - 1, lows - 1)), dma((chips, n_sp)),
            dma((highs - 1,)), dma((lows - 1,)), dma((highs - 1, lows - 1)), dma((n_sp,)),
            dma((chips, groups, 2)), dma((n_tp * groups,)),
        ],
        compiler_params=pltpu.CompilerParams(
            collective_id=0, has_side_effects=True, vmem_limit_bytes=60 << 20
        ),
        name="fused",
    )(
        latent, context, condition[None], context_condition[None], norm_gain[None],
        shift_weight, scale_weight, gate_weight, query_weight, key_weight, value_weight,
        query_gain[None], key_gain[None], output_weight,
    )


def solution(mesh):
    in_specs = (
        P(("sp", "tp"), None), P("sp", None), P(), P(), P(),
        P("sp", "tp"), P("sp", "tp"), P("sp", "tp"),
        P(None, "tp"), P(None, "tp"), P(None, "tp"), P(), P(), P(),
    )
    return jax.shard_map(
        on_device, mesh=mesh, in_specs=in_specs, out_specs=P(("sp", "tp"), None), check_vma=False
    )
```

```python
import functools
import math

import jax
import jax.numpy as jnp
from jax import lax
from jax.experimental import pallas as pl
from jax.experimental.pallas import tpu as pltpu
from jax.sharding import PartitionSpec as P

SPAN = 64
GRID_W = 64
QUARTER = SPAN // 4
LAG = 6
PIECES = 2
LOG2E = 1.4426950408889634
MESH = pl.DeviceIdType.MESH
VMEM = pl.BlockSpec(memory_space=pltpu.VMEM)
ANY = pl.BlockSpec(memory_space=pl.ANY)
F32 = jnp.float32
BF16 = jnp.bfloat16

epsilon = 1e-06
rope_base = 10000.0


def kernel(
    n_sp, n_tp, lows, offset, split,
    latent_hbm, context_hbm, cond, ctx_cond, norm_gain, w_shift_hbm, w_scale_hbm, w_gate_hbm,
    w_q_hbm, w_k_hbm, w_v_hbm, q_gain, k_gain, w_out_hbm,
    out,
    lat, context, w_mod, w_all, w_side, w_out, part, parts, mods, part_g, parts_g, mods_g,
    coef, hidden, table, gain_q, gain_k, q_send, q_raw, kv_send, ctx_send, ctx_all, q_all, kv_all,
    k_nat, peak, acc, attended, received,
    load, lat_send, lat_fwd, lat_recv, sp_send, sp_recv, tp_send, tp_recv,
    q_ssem, q_rsem, z_send, y_send, f_send, kv_recv,
    cz_send, cy_send, cf_send, c_recv, at_send, at_recv,
):
    sp, tp = lax.axis_index("sp"), lax.axis_index("tp")
    chips = n_tp // 2
    highs = n_sp // lows
    low, high = lax.rem(sp, lows), sp // lows
    x, core = tp // 2, lax.rem(tp, 2)
    twin = tp + 1 - 2 * core
    width = lat.shape[1]
    own_rows = width // 2
    model = lat.shape[2]
    tok = chips * width
    ctx_rows = context.shape[0]
    groups = kv_send.shape[1]
    heads = q_send.shape[2]
    q_width = groups * heads * SPAN
    kv_width = groups * SPAN
    row_slab, columns = w_mod.shape[1], w_mod.shape[2]
    bands = columns // 128
    g = lax.rem(high, groups)
    base = high - g
    ctx_slots = n_sp * ctx_rows // width
    ctx_first = chips * n_sp
    step = own_rows // PIECES
    part_width = width // split

    def dev(z, y):
        return z * lows + y

    def remote(src, dst, ssem, rsem, peer):
        return pltpu.make_async_remote_copy(
            src_ref=src, dst_ref=dst, send_sem=ssem, recv_sem=rsem,
            device_id=peer, device_id_type=MESH,
        )

    def lanes_of(d, p):
        if d == 0 or split == 1:
            return slice(0, width)
        return slice(p * part_width, (p + 1) * part_width)

    def parts_in(d):
        return 1 if d == 0 else split

    barrier = pltpu.get_barrier_semaphore()
    peers = [(lax.rem(sp + d, n_sp), tp) for d in range(1, n_sp)]
    peers += [(sp, lax.rem(tp + d, n_tp)) for d in range(1, n_tp)]
    for r in range(1, groups):
        mate = dev(base + lax.rem(g + r, groups), low)
        peers += [(mate, lax.rem(tp + d, n_tp)) for d in range(1, n_tp)]
    for p in peers:
        pl.semaphore_signal(barrier, inc=1, device_id=p, device_id_type=MESH)

    mine_rows = pl.ds(pl.multiple_of(core * own_rows, own_rows), own_rows)
    pairs = [
        (w_shift_hbm, w_mod.at[0]), (w_scale_hbm, w_mod.at[1]),
        (latent_hbm, lat.at[x, mine_rows, :]), (w_gate_hbm, w_mod.at[2]),
        (context_hbm, context), (w_q_hbm, w_all.at[:, 0:q_width]),
    ]
    if kv_width % 128 == 0:
        pairs += [
            (w_k_hbm, w_all.at[:, q_width : q_width + kv_width]),
            (w_v_hbm, w_all.at[:, q_width + kv_width :]),
        ]
    else:
        pairs += [(w_k_hbm, w_side.at[0]), (w_v_hbm, w_side.at[1])]
    pairs.append((w_out_hbm, w_out))
    loads = [pltpu.make_async_copy(s, d, load.at[i]) for i, (s, d) in enumerate(pairs)]
    for c in loads[:-1]:
        c.start()

    def slab(ref):
        if row_slab % 128 == 0:
            return ref[:, pl.ds(pl.multiple_of(sp * row_slab, 128), row_slab)]
        per = 128 // row_slab
        window = ref[:, pl.ds(pl.multiple_of(sp // per * 128, 128), 128)]
        pick = lax.rem(sp, per)
        result = window
        for k in range(1, per):
            result = jnp.where(pick == k, pltpu.roll(window, 128 - k * row_slab, 1), result)
        return result[:, :row_slab]

    v = jnp.concatenate([slab(cond), slab(ctx_cond)], axis=0)
    act = (v / (1.0 + jnp.exp(-v))).astype(BF16)
    part_g[...] = jnp.zeros_like(part_g)
    for i in range(2):
        loads[i].wait()
        r = jnp.dot(act, w_mod[i], preferred_element_type=F32)
        for row in range(2):
            for k in range(bands):
                at = (2 * i + row) * bands + k
                part[at : at + 1, :] = r[row : row + 1, k * 128 : (k + 1) * 128]
    loads[2].wait()
    pl.semaphore_wait(barrier, len(peers))

    def rows_of(tile, piece):
        chip, half = tile // 2, lax.rem(tile, 2)
        start = pl.multiple_of(half * own_rows + piece * step, step)
        return lat.at[chip, pl.ds(start, step), :]

    def row_copy(tile, piece, ssem, peer):
        return remote(
            rows_of(tile, piece), rows_of(tile, piece), ssem, lat_recv.at[tile, piece], (sp, peer)
        )

    lat_sends = []

    def send_piece(piece):
        for d in range(1, chips):
            c = row_copy(tp, piece, lat_send.at[d, piece], lax.rem(tp + 2 * d, n_tp))
            c.start()
            lat_sends.append(c)

    sp_copies = []
    for d in range(1, n_sp):
        c = remote(
            part, parts.at[sp], sp_send.at[0, d - 1], sp_recv.at[0, d - 1],
            (lax.rem(sp + d, n_sp), tp),
        )
        c.start()
        sp_copies.append(c)
    send_piece(0)
    for piece in range(PIECES):
        c = row_copy(tp, piece, lat_send.at[0, piece], twin)
        c.start()
        lat_sends.append(c)
    parts[sp] = part[...]

    loads[3].wait()
    r = jnp.dot(act, w_mod[2], preferred_element_type=F32)
    for k in range(bands):
        part_g[k : k + 1, :] = r[0:1, k * 128 : (k + 1) * 128]
    parts_g[sp] = part_g[...]
    loads[-1].start()
    for d in range(chips):
        chip = lax.rem(x - d + chips, chips)
        lane = lax.broadcasted_iota(jnp.int32, (QUARTER, width), 1)
        if parts_in(d) > 1:
            lane = lane // step % 2 * own_rows + lane // part_width * step + lane % step
        place = sp * tok + chip * width + lane
        turn = lax.broadcasted_iota(jnp.int32, (QUARTER, width), 0).astype(F32)
        freq = jnp.exp(turn * (-math.log(rope_base) / QUARTER))
        by_row = (place // GRID_W).astype(F32) * freq
        by_col = (place % GRID_W).astype(F32) * freq
        table[d, 0:QUARTER, :] = jnp.cos(by_row)
        table[d, QUARTER : 2 * QUARTER, :] = jnp.sin(by_row)
        table[d, 2 * QUARTER : 3 * QUARTER, :] = jnp.cos(by_col)
        table[d, 3 * QUARTER :, :] = jnp.sin(by_col)
    k_pair = jnp.concatenate([k_gain[...], k_gain[...]], axis=1)
    for ref, dst in ((q_gain, gain_q), (k_gain, gain_k)):
        row = jnp.concatenate([ref[...], ref[...]], axis=1)
        square = jnp.transpose(jnp.broadcast_to(row, (128, 128)))[0:SPAN, :]
        for c in range(0, width, 128):
            dst[:, c : c + 128] = square
    peak[...] = jnp.full_like(peak, -1e30)
    acc[...] = jnp.zeros_like(acc)
    kv_all[:, 2 * SPAN :, :] = jnp.ones((kv_all.shape[0], 16, width), BF16)

    for c in sp_copies:
        c.wait()
    summed = parts[0]
    for j in range(1, n_sp):
        summed = summed + parts[j]
    part[...] = summed
    mods[tp] = summed
    tp_copies = []
    for d in range(1, n_tp):
        c = remote(
            part, mods.at[tp], tp_send.at[0, d - 1], tp_recv.at[0, d - 1],
            (sp, lax.rem(tp + d, n_tp)),
        )
        c.start()
        tp_copies.append(c)
    for piece in range(1, PIECES):
        send_piece(piece)
    gate_copies = []
    for d in range(1, n_sp):
        c = remote(
            part_g, parts_g.at[sp], sp_send.at[1, d - 1], sp_recv.at[1, d - 1],
            (lax.rem(sp + d, n_sp), tp),
        )
        c.start()
        gate_copies.append(c)
    for c in loads[4:-1]:
        c.wait()
    if kv_width % 128 != 0:
        w_all[:, q_width:] = jnp.concatenate([w_side[0], w_side[1]], axis=1)
    for piece in range(PIECES):
        row_copy(twin, piece, lat_send.at[0, 0], twin).wait_recv()
    for c in tp_copies:
        c.wait()
    for t in range(n_tp):
        for k in range(bands):
            cols = slice(t * columns + k * 128, t * columns + (k + 1) * 128)
            for row in range(2):
                at = (2 + row) * bands + k
                coef[row : row + 1, cols] = norm_gain[:, cols] * (1.0 + mods[t, at : at + 1, :])
                at = row * bands + k
                coef[2 + row : 3 + row, cols] = mods[t, at : at + 1, :]

    block = 16

    def modulate(read, rows, first, row):
        def body(i, carry):
            w = read(i * block).astype(F32)
            inv = lax.rsqrt(jnp.sum(w * w, axis=-1, keepdims=True) / model + epsilon)
            y = w * inv * coef[row : row + 1, :] + coef[2 + row : 3 + row, :]
            hidden[pl.ds(pl.multiple_of(first + i * block, block), block), :] = y.astype(BF16)
            return carry

        lax.fori_loop(0, rows // block, body, 0, unroll=min(4, rows // block))

    far = [d for d in range(2, highs)] if highs > 2 else []
    z_order = far[:1] + [1] + far[1:] if highs > 1 else []
    tail_sends = []

    def begin(c):
        c.start()
        tail_sends.append(c)

    def ctx_copy(head, src, ssem, z, y):
        return remote(ctx_send.at[head], ctx_all.at[src], ssem, c_recv.at[src], (dev(z, y), tp))

    def context_step():
        modulate(
            lambda i: context[pl.ds(pl.multiple_of(i, block), block), :], ctx_rows, 0, 1
        )
        raw = jnp.dot(hidden[0:ctx_rows, :], w_all[:, q_width:], preferred_element_type=F32)
        if groups == 2:
            k, val = raw[:, :kv_width], raw[:, kv_width:]
            first = lax.broadcasted_iota(jnp.int32, k.shape, 1) < SPAN
            sq = k * k
            s0 = jnp.sum(jnp.where(first, sq, 0.0), axis=-1, keepdims=True)
            s1 = jnp.sum(jnp.where(first, 0.0, sq), axis=-1, keepdims=True)
            scale = jnp.where(
                first, lax.rsqrt(s0 / SPAN + epsilon), lax.rsqrt(s1 / SPAN + epsilon)
            )
            k = k * scale * k_pair
            ctx_send[0] = jnp.where(first, k, pltpu.roll(val, SPAN, 1)).astype(BF16)
            ctx_send[1] = jnp.where(first, pltpu.roll(k, SPAN, 1), val).astype(BF16)
        else:
            first = lax.broadcasted_iota(jnp.int32, raw.shape, 1) < SPAN
            s0 = jnp.sum(jnp.where(first, raw * raw, 0.0), axis=-1, keepdims=True)
            k = raw * lax.rsqrt(s0 / SPAN + epsilon) * k_pair
            ctx_send[0] = jnp.where(first, k, raw).astype(BF16)
        for dz in z_order:
            z = lax.rem(high + dz, highs)
            begin(ctx_copy(lax.rem(z, groups), sp, cz_send.at[dz - 1], z, low))
        for dl in range(1, lows):
            begin(ctx_copy(g, sp, cy_send.at[dl - 1], high, lax.rem(low + dl, lows)))
        ctx_all[sp] = ctx_send[g]

    def finish(raw_head, gain, d, lanes):
        n = lanes.stop - lanes.start
        inv = lax.rsqrt(jnp.sum(raw_head * raw_head, axis=0, keepdims=True) / SPAN + epsilon)
        y = raw_head * inv * gain[:, 0:n]
        a1, b1 = y[0:QUARTER], y[QUARTER : 2 * QUARTER]
        a2, b2 = y[2 * QUARTER : 3 * QUARTER], y[3 * QUARTER :]
        cr, sr = table[d, 0:QUARTER, lanes], table[d, QUARTER : 2 * QUARTER, lanes]
        cc, sc = table[d, 2 * QUARTER : 3 * QUARTER, lanes], table[d, 3 * QUARTER :, lanes]
        return jnp.concatenate(
            [a1 * cr - b1 * sr, b1 * cr + a1 * sr, a2 * cc - b2 * sc, b2 * cc + a2 * sc], axis=0
        )

    def q_copy(d, p, group, ssem, z):
        lanes = lanes_of(d, p)
        return remote(
            q_send.at[d, group, :, :, lanes], q_raw.at[d, g, :, :, lanes], ssem,
            q_rsem.at[d, p, g], (dev(z, low), tp),
        )

    def q_store(d, group, value):
        f = value.astype(F32) * LOG2E
        hi = f.astype(BF16)
        q_all[d * groups + group, :, 0:SPAN, :] = hi
        q_all[d * groups + group, :, SPAN:, :] = (f - hi.astype(F32)).astype(BF16)

    def q_own(d):
        q_store(d, g, q_send[d, g])

    def q_arrive(d):
        for r in range(1, groups):
            other = lax.rem(g + r, groups)
            for p in range(parts_in(d)):
                lanes = lanes_of(d, p)
                dst = q_raw.at[d, other, :, :, lanes]
                remote(
                    dst, dst, q_ssem.at[d, 0, 0], q_rsem.at[d, p, other], (dev(base + other, low), tp)
                ).wait_recv()
            q_store(d, other, q_raw[d, other])

    def kv_copy(src_ref, d, p, src, ssem, z, y):
        lanes = lanes_of(d, p)
        return remote(
            src_ref, kv_all.at[d * n_sp + src, 0 : 2 * SPAN, lanes], ssem, kv_recv.at[d, p, src],
            (dev(z, y), tp),
        )

    def key_rows(slot, lanes):
        k = kv_all[slot, 0:SPAN, lanes]
        k_nat[slot, lanes, :] = jnp.transpose(jnp.concatenate([k, k], axis=0))

    def project(d, p):
        chip = lax.rem(x - d + chips, chips)
        lanes = lanes_of(d, p)
        n = lanes.stop - lanes.start
        if n == width:
            modulate(
                lambda i: lat[chip, pl.ds(pl.multiple_of(i, block), block), :], width, 0, 0
            )
        else:
            for half in range(2):
                at = half * own_rows + p * step
                modulate(
                    lambda i: lat[chip, pl.ds(pl.multiple_of(at + i, block), block), :],
                    step, half * step, 0,
                )
        flat = jnp.dot(hidden[0:n, :], w_all[...], preferred_element_type=F32)
        up = jnp.transpose(flat)
        for j in range(groups):
            r = q_width + j * SPAN
            kv_send[d, j, 0:SPAN, lanes] = finish(up[r : r + SPAN], gain_k, d, lanes).astype(BF16)
            r = q_width + kv_width + j * SPAN
            kv_send[d, j, SPAN:, lanes] = up[r : r + SPAN].astype(BF16)
            for h in range(heads):
                r = (j * heads + h) * SPAN
                y = finish(up[r : r + SPAN], gain_q, d, lanes)
                q_send[d, j, h, :, lanes] = (y * SPAN ** (-0.5)).astype(BF16)
        for r in range(1, groups):
            other = lax.rem(g + r, groups)
            begin(q_copy(d, p, other, q_ssem.at[d, p, r - 1], base + other))
        for dz in z_order:
            z = lax.rem(high + dz, highs)
            src = kv_send.at[d, lax.rem(z, groups), :, lanes]
            begin(kv_copy(src, d, p, sp, z_send.at[d, p, dz - 1], z, low))
        for dl in range(1, lows):
            y = lax.rem(low + dl, lows)
            src = kv_send.at[d, g, :, lanes]
            begin(kv_copy(src, d, p, sp, y_send.at[d, p, dl - 1], high, y))
        kv_all[d * n_sp + sp, 0 : 2 * SPAN, lanes] = kv_send[d, g, :, lanes]
        key_rows(d * n_sp + sp, lanes)

    def column(d, p, dz):
        src = dev(lax.rem(high - dz + highs, highs), low)
        slot = d * n_sp + src
        lanes = lanes_of(d, p)
        here = kv_all.at[slot, 0 : 2 * SPAN, lanes]
        kv_copy(here, d, p, src, z_send.at[0, 0, 0], high, low).wait_recv()
        for dl in range(1, lows):
            y = lax.rem(low + dl, lows)
            begin(kv_copy(here, d, p, src, f_send.at[d, p, dz - 1, dl - 1], high, y))
        key_rows(slot, lanes)

    def ctx_column(dz):
        src = dev(lax.rem(high - dz + highs, highs), low)
        ctx_copy(0, src, cz_send.at[0], high, low).wait_recv()
        for dl in range(1, lows):
            y = lax.rem(low + dl, lows)
            begin(
                remote(
                    ctx_all.at[src], ctx_all.at[src], cf_send.at[dz - 1, dl - 1],
                    c_recv.at[src], (dev(high, y), tp),
                )
            )

    def side(d, dz, dl):
        src = dev(lax.rem(high - dz + highs, highs), lax.rem(low - dl + lows, lows))
        slot = d * n_sp + src
        for p in range(parts_in(d)):
            lanes = lanes_of(d, p)
            here = kv_all.at[slot, 0 : 2 * SPAN, lanes]
            kv_copy(here, d, p, src, z_send.at[0, 0, 0], high, low).wait_recv()
            key_rows(slot, lanes)

    def ctx_ready():
        for dl in range(1, lows):
            for dz in range(highs):
                src = dev(lax.rem(high - dz + highs, highs), lax.rem(low - dl + lows, lows))
                ctx_copy(0, src, cz_send.at[0], high, low).wait_recv()
        per = width // ctx_rows
        for c in range(ctx_slots):
            piece = ctx_all[c * per : (c + 1) * per].reshape(width, 2 * SPAN)
            kv_all[ctx_first + c, 0 : 2 * SPAN, :] = jnp.transpose(piece)
            key_rows(ctx_first + c, slice(0, width))

    def slot_of(d, dz, dl):
        return d * n_sp + dev(
            lax.rem(high - dz + highs, highs), lax.rem(low - dl + lows, lows)
        )

    def attend(items):
        items = [(s, t, h) for s, t in items for h in range(heads)]
        n = len(items)
        scores = {}

        def score(i):
            s, t, h = items[i]
            r = jnp.dot(k_nat[s], q_all[t, h], preferred_element_type=F32)
            if isinstance(s, int) and s >= ctx_first:
                r = r + offset * LOG2E
            scores[i] = r

        for i in range(min(LAG, n)):
            score(i)
        for i in range(n):
            if i + LAG < n:
                score(i + LAG)
            slot, t, h = items[i]
            s = scores.pop(i)
            old = peak[t, h, 0:1, :]
            top = jnp.maximum(jnp.max(s, axis=0, keepdims=True), old)
            shrink = jnp.exp2(old - top)
            e = jnp.exp2(s - top).astype(BF16)
            peak[t, h] = jnp.broadcast_to(top, (8, width))
            w = jnp.dot(kv_all[slot, SPAN:, :], e, preferred_element_type=F32)
            acc[t, h] = acc[t, h] * shrink + w

    def attend_range(first, count, tile_list):
        per = math.gcd(max(1, 8 // len(tile_list)), count)

        def body(i, carry):
            attend([(first + i * per + u, t) for u in range(per) for t in tile_list])
            return carry

        lax.fori_loop(0, count // per, body, 0)

    def fetch(d, piece):
        chip = lax.rem(x - d + chips, chips)
        near = 2 * chip + core
        row_copy(near, piece, lat_send.at[0, 0], twin).wait_recv()
        begin(row_copy(near, piece, lat_fwd.at[d - 1, piece], twin))

    def fetch_back(d, piece):
        chip = lax.rem(x - d + chips, chips)
        row_copy(2 * chip + 1 - core, piece, lat_send.at[0, 0], twin).wait_recv()

    copies = []

    def deliver(d, r):
        chip = lax.rem(x - d + chips, chips)
        j = lax.rem(g + r, groups)
        t = d * groups + j
        rows = []
        for h in range(heads):
            inv = 1.0 / acc[t, h, SPAN : SPAN + 1, :]
            rows.append(acc[t, h, 0:SPAN, :] * inv)
        turned = jnp.transpose(jnp.concatenate(rows, axis=0)).astype(BF16)
        if parts_in(d) == 1:
            attended[d, r] = turned
        else:
            for p in range(split):
                for half in range(2):
                    at = half * own_rows + p * step
                    took = p * part_width + half * step
                    attended[d, r, at : at + step, :] = turned[took : took + step]
        for rc in range(2):
            half = lax.rem(core + rc, 2)
            src = attended.at[d, r, pl.ds(pl.multiple_of(half * own_rows, own_rows), own_rows), :]
            if d == 0 and r == 0 and rc == 0:
                received[tp * groups + g] = src[...]
            else:
                c = remote(
                    src, received.at[tp * groups + g], at_send.at[d, r, rc],
                    at_recv.at[tp * groups + g], (dev(base + j, low), 2 * chip + half),
                )
                c.start()
                copies.append(c)

    def gates():
        for c in gate_copies:
            c.wait()
        whole = parts_g[0]
        for j in range(1, n_sp):
            whole = whole + parts_g[j]
        part_g[...] = whole
        mods_g[tp] = whole
        result = []
        for d in range(1, n_tp):
            c = remote(
                part_g, mods_g.at[tp], tp_send.at[1, d - 1], tp_recv.at[1, d - 1],
                (sp, lax.rem(tp + d, n_tp)),
            )
            c.start()
            result.append(c)
        return result

    def tile_of(d, r):
        return d * groups + lax.rem(g + r, groups)

    if chips == 2 and split == 2 and n_sp == 8 and groups == 2:
        project(0, 0)
        fetch(1, 0)
        context_step()
        fetch_back(1, 0)
        project(1, 0)
        gate_out = gates()
        early = [tile_of(0, 0), tile_of(0, 1)]
        q_own(0)
        q_arrive(0)
        za, zb, zc = z_order
        attend([(slot_of(0, 0, 0), t) for t in early])
        column(0, 0, za)
        column(0, 0, zb)
        fetch(1, 1)
        attend([(slot_of(0, dz, 0), t) for dz in (za, zb) for t in early])
        column(0, 0, zc)
        for dz in z_order:
            ctx_column(dz)
        fetch_back(1, 1)
        project(1, 1)
        q_own(1)
        side(0, 0, 1)
        attend([(slot_of(0, zc, 0), t) for t in early] + [(slot_of(0, 0, 1), t) for t in early])
        column(1, 0, za)
        side(0, za, 1)
        side(0, zb, 1)
        attend([(slot_of(0, dz, 1), t) for dz in (za, zb) for t in early])
        column(1, 0, zb)
        column(1, 0, zc)
        ctx_ready()
        own_b, mate_b = tile_of(1, 0), tile_of(1, 1)
        ctx = range(ctx_first, ctx_first + ctx_slots)
        attend([(s, t) for s in ctx for t in early + [own_b]])
        column(1, 1, za)
        side(0, zc, 1)
        attend(
            [(slot_of(0, zc, 1), t) for t in early]
            + [(s, own_b) for s in range(0, n_sp // 2)]
        )
        column(1, 1, zb)
        attend([(s, own_b) for s in range(n_sp // 2, n_sp)])
        column(1, 1, zc)
        q_arrive(1)
        attend([(s, mate_b) for s in list(range(n_sp)) + list(ctx)])
        every = [tile_of(0, 1), mate_b, own_b, tile_of(0, 0)]
        attend([(slot_of(1, dz, 0), t) for dz in (0, za) for t in every])
        attend([(slot_of(1, dz, 0), t) for dz in (zb, zc) for t in every])
        last = [0] + z_order
        for dz in last:
            side(1, dz, 1)
        for (d, r), t in zip(((0, 1), (1, 1), (1, 0), (0, 0)), every):
            attend([(slot_of(1, dz, 1), t) for dz in last])
            deliver(d, r)
    else:
        context_step()
        for d in range(chips):
            if d > 0:
                for piece in range(PIECES):
                    fetch(d, piece)
                for piece in range(PIECES):
                    fetch_back(d, piece)
            for p in range(parts_in(d)):
                project(d, p)
            q_own(d)
        gate_out = gates()
        for dz in z_order:
            ctx_column(dz)
        for d in range(chips):
            for p in range(parts_in(d)):
                for dz in z_order:
                    column(d, p, dz)
            q_arrive(d)
        ctx_ready()
        for d in range(chips):
            for dl in range(1, lows):
                for dz in range(highs):
                    side(d, dz, dl)
        for d in range(chips):
            for r in range(groups):
                t = tile_of(d, r)
                attend_range(0, ctx_first, [t])
                attend([(s, t) for s in range(ctx_first, ctx_first + ctx_slots)])
                deliver(d, r)

    loads[-1].wait()
    for c in gate_out:
        c.wait()
    for rt in range(n_tp):
        for r in range(groups):
            if rt == 0 and r == 0:
                continue
            who = lax.rem(tp + rt, n_tp) * groups + lax.rem(g + r, groups)
            remote(
                received.at[who], received.at[who], at_send.at[0, 0, 1], at_recv.at[who],
                (sp, twin),
            ).wait_recv()
    rows = jnp.concatenate([received[s] for s in range(n_tp * groups)], axis=1)
    for t in range(n_tp):
        cols = slice(t * columns, (t + 1) * columns)
        gate = jnp.concatenate([mods_g[t, k : k + 1, :] for k in range(bands)], axis=1)
        branch = jnp.dot(rows, w_out[:, cols], preferred_element_type=F32)
        out[:, cols] = (lat[x, mine_rows, cols].astype(F32) + gate * branch).astype(BF16)
    for c in lat_sends + tail_sends + copies:
        c.wait_send()


def on_device(
    latent, context, condition, context_condition, norm_gain, shift_weight, scale_weight,
    gate_weight, query_weight, key_weight, value_weight, query_gain, key_gain, output_weight,
):
    n_sp, n_tp = lax.axis_size("sp"), lax.axis_size("tp")
    row_slab, columns = shift_weight.shape
    own_rows, model = latent.shape
    ctx_rows = context.shape[0]
    tok = own_rows * n_tp
    q_width, kv_width = query_weight.shape[1], key_weight.shape[1]
    groups = kv_width // SPAN
    heads = q_width // SPAN // groups
    chips = n_tp // 2
    width = 2 * own_rows
    lows = 2 ** (int(math.log2(n_sp)) // 2)
    highs = n_sp // lows
    slots = chips * n_sp + n_sp * ctx_rows // width
    n_tiles = chips * groups
    split = 2 if width // 2 % 128 == 0 else 1
    bands = columns // 128
    offset = math.log(tok / (2.0 * ctx_rows))
    dma = pltpu.SemaphoreType.DMA
    return pl.pallas_call(
        functools.partial(kernel, n_sp, n_tp, lows, offset, split),
        out_shape=jax.ShapeDtypeStruct(latent.shape, BF16),
        in_specs=[ANY] * 2 + [VMEM] * 3 + [ANY] * 6 + [VMEM] * 2 + [ANY],
        out_specs=VMEM,
        scratch_shapes=[
            pltpu.VMEM((chips, width, model), BF16),
            pltpu.VMEM(context.shape, BF16),
            pltpu.VMEM((3, row_slab, columns), BF16),
            pltpu.VMEM((model, q_width + 2 * kv_width), BF16),
            pltpu.VMEM((2,) + (key_weight.shape if kv_width % 128 else (16, 128)), BF16),
            pltpu.VMEM(output_weight.shape, BF16),
            pltpu.VMEM((4 * bands, 128), F32),
            pltpu.VMEM((n_sp, 4 * bands, 128), F32),
            pltpu.VMEM((n_tp, 4 * bands, 128), F32),
            pltpu.VMEM((8, 128), F32),
            pltpu.VMEM((n_sp, 8, 128), F32),
            pltpu.VMEM((n_tp, 8, 128), F32),
            pltpu.VMEM((8, model), F32),
            pltpu.VMEM((width, model), BF16),
            pltpu.VMEM((chips, SPAN, width), F32),
            pltpu.VMEM((SPAN, width), F32),
            pltpu.VMEM((SPAN, width), F32),
            pltpu.VMEM((chips, groups, heads, SPAN, width), BF16),
            pltpu.VMEM((chips, groups, heads, SPAN, width), BF16),
            pltpu.VMEM((chips, groups, 2 * SPAN, width), BF16),
            pltpu.VMEM((groups, ctx_rows, 2 * SPAN), BF16),
            pltpu.VMEM((n_sp, ctx_rows, 2 * SPAN), BF16),
            pltpu.VMEM((n_tiles, heads, 2 * SPAN, width), BF16),
            pltpu.VMEM((slots, 2 * SPAN + 16, width), BF16),
            pltpu.VMEM((slots, width, 2 * SPAN), BF16),
            pltpu.VMEM((n_tiles, heads, 8, width), F32),
            pltpu.VMEM((n_tiles, heads, SPAN + 16, width), F32),
            pltpu.VMEM((chips, groups, width, 2 * SPAN), BF16),
            pltpu.VMEM((n_tp * groups, own_rows, 2 * SPAN), BF16),
            dma((9,)), dma((chips, PIECES)), dma((max(chips - 1, 1), PIECES)), dma((n_tp, PIECES)),
            dma((2, n_sp - 1)), dma((2, n_sp - 1)), dma((2, n_tp - 1)), dma((2, n_tp - 1)),
            dma((chips, split, max(groups - 1, 1))), dma((chips, split, groups)),
            dma((chips, split, highs - 1)), dma((chips, split, lows - 1)),
            dma((chips, split, highs - 1, lows - 1)), dma((chips, split, n_sp)),
            dma((highs - 1,)), dma((lows - 1,)), dma((highs - 1, lows - 1)), dma((n_sp,)),
            dma((chips, groups, 2)), dma((n_tp * groups,)),
        ],
        compiler_params=pltpu.CompilerParams(
            collective_id=0, has_side_effects=True, vmem_limit_bytes=60 << 20
        ),
        name="fused",
    )(
        latent, context, condition[None], context_condition[None], norm_gain[None],
        shift_weight, scale_weight, gate_weight, query_weight, key_weight, value_weight,
        query_gain[None], key_gain[None], output_weight,
    )


def solution(mesh):
    in_specs = (
        P(("sp", "tp"), None), P("sp", None), P(), P(), P(),
        P("sp", "tp"), P("sp", "tp"), P("sp", "tp"),
        P(None, "tp"), P(None, "tp"), P(None, "tp"), P(), P(), P(),
    )
    return jax.shard_map(
        on_device, mesh=mesh, in_specs=in_specs, out_specs=P(("sp", "tp"), None), check_vma=False
    )
```

```python
import functools
import math

import jax
import jax.numpy as jnp
from jax import lax
from jax.experimental import pallas as pl
from jax.experimental.pallas import tpu as pltpu
from jax.sharding import PartitionSpec as P

SPAN = 64
GRID_W = 64
QUARTER = SPAN // 4
LAG = 4
OWE = 0
PIECES = 2
LOG2E = 1.4426950408889634
MESH = pl.DeviceIdType.MESH
VMEM = pl.BlockSpec(memory_space=pltpu.VMEM)
ANY = pl.BlockSpec(memory_space=pl.ANY)
F32 = jnp.float32
BF16 = jnp.bfloat16

epsilon = 1e-06
rope_base = 10000.0


def kernel(
    n_sp, n_tp, lows, offset, split,
    latent_hbm, context_hbm, cond_hbm, ctx_cond_hbm, norm_gain_hbm, w_shift_hbm, w_scale_hbm,
    w_gate_hbm, w_q_hbm, w_k_hbm, w_v_hbm, q_gain_hbm, k_gain_hbm, w_out_hbm,
    out, cond, ctx_cond, norm_gain, q_gain, k_gain,
    lat, context, w_mod, w_all, w_side, w_out, part, parts, mods, part_g, parts_g, mods_g,
    coef, hidden, table, gain_q, gain_k, q_send, q_raw, kv_send, ctx_send, ctx_all, q_all, kv_all,
    k_nat, peak, acc, attended, received,
    load, lat_send, lat_fwd, lat_recv, sp_send, sp_recv, tp_send, tp_recv,
    q_ssem, q_rsem, z_send, y_send, f_send, kv_recv,
    cz_send, cy_send, cf_send, c_recv, at_send, at_recv, small_sem,
):
    sp, tp = lax.axis_index("sp"), lax.axis_index("tp")
    chips = n_tp // 2
    highs = n_sp // lows
    low, high = lax.rem(sp, lows), sp // lows
    x, core = tp // 2, lax.rem(tp, 2)
    twin = tp + 1 - 2 * core
    width = lat.shape[1]
    own_rows = width // 2
    model = lat.shape[2]
    tok = chips * width
    ctx_rows = context.shape[0]
    groups = kv_send.shape[1]
    heads = q_send.shape[2]
    q_width = groups * heads * SPAN
    kv_width = groups * SPAN
    row_slab, columns = w_mod.shape[1], w_mod.shape[2]
    bands = columns // 128
    g = lax.rem(high, groups)
    base = high - g
    ctx_slots = n_sp * ctx_rows // width
    ctx_first = chips * n_sp
    step = own_rows // PIECES
    part_width = width // split

    def dev(z, y):
        return z * lows + y

    def remote(src, dst, ssem, rsem, peer):
        return pltpu.make_async_remote_copy(
            src_ref=src, dst_ref=dst, send_sem=ssem, recv_sem=rsem,
            device_id=peer, device_id_type=MESH,
        )

    def lanes_of(d, p):
        if d == 0 or split == 1:
            return slice(0, width)
        return slice(p * part_width, (p + 1) * part_width)

    def parts_in(d):
        return 1 if d == 0 else split

    barrier = pltpu.get_barrier_semaphore()
    peers = [(lax.rem(sp + d, n_sp), tp) for d in range(1, n_sp)]
    peers += [(sp, lax.rem(tp + d, n_tp)) for d in range(1, n_tp)]
    for r in range(1, groups):
        mate = dev(base + lax.rem(g + r, groups), low)
        peers += [(mate, lax.rem(tp + d, n_tp)) for d in range(1, n_tp)]
    for p in peers:
        pl.semaphore_signal(barrier, inc=1, device_id=p, device_id_type=MESH)

    mine_rows = pl.ds(pl.multiple_of(core * own_rows, own_rows), own_rows)
    pairs = [
        (w_shift_hbm, w_mod.at[0]), (w_scale_hbm, w_mod.at[1]),
        (latent_hbm, lat.at[x, mine_rows, :]), (w_gate_hbm, w_mod.at[2]),
        (context_hbm, context), (w_q_hbm, w_all.at[:, 0:q_width]),
    ]
    if kv_width % 128 == 0:
        pairs += [
            (w_k_hbm, w_all.at[:, q_width : q_width + kv_width]),
            (w_v_hbm, w_all.at[:, q_width + kv_width :]),
        ]
    else:
        pairs += [(w_k_hbm, w_side.at[0]), (w_v_hbm, w_side.at[1])]
    pairs.append((w_out_hbm, w_out))
    small = [
        pltpu.make_async_copy(s, d, small_sem.at[i])
        for i, (s, d) in enumerate(
            (
                (cond_hbm, cond), (ctx_cond_hbm, ctx_cond), (norm_gain_hbm, norm_gain),
                (q_gain_hbm, q_gain), (k_gain_hbm, k_gain),
            )
        )
    ]
    for c in small:
        c.start()
    loads = [pltpu.make_async_copy(s, d, load.at[i]) for i, (s, d) in enumerate(pairs)]
    for c in loads[:-1]:
        c.start()

    def slab(ref):
        if row_slab % 128 == 0:
            return ref[:, pl.ds(pl.multiple_of(sp * row_slab, 128), row_slab)]
        per = 128 // row_slab
        window = ref[:, pl.ds(pl.multiple_of(sp // per * 128, 128), 128)]
        pick = lax.rem(sp, per)
        result = window
        for k in range(1, per):
            result = jnp.where(pick == k, pltpu.roll(window, 128 - k * row_slab, 1), result)
        return result[:, :row_slab]

    for c in small:
        c.wait()
    v = jnp.concatenate([slab(cond), slab(ctx_cond)], axis=0)
    act = (v / (1.0 + jnp.exp(-v))).astype(BF16)
    part_g[...] = jnp.zeros_like(part_g)
    for i in range(2):
        loads[i].wait()
        r = jnp.dot(act, w_mod[i], preferred_element_type=F32)
        for row in range(2):
            for k in range(bands):
                at = (2 * i + row) * bands + k
                part[at : at + 1, :] = r[row : row + 1, k * 128 : (k + 1) * 128]
    loads[2].wait()
    pl.semaphore_wait(barrier, len(peers))

    def rows_of(tile, piece):
        chip, half = tile // 2, lax.rem(tile, 2)
        start = pl.multiple_of(half * own_rows + piece * step, step)
        return lat.at[chip, pl.ds(start, step), :]

    def row_copy(tile, piece, ssem, peer):
        return remote(
            rows_of(tile, piece), rows_of(tile, piece), ssem, lat_recv.at[tile, piece], (sp, peer)
        )

    lat_sends = []

    def send_piece(piece):
        for d in range(1, chips):
            c = row_copy(tp, piece, lat_send.at[d, piece], lax.rem(tp + 2 * d, n_tp))
            c.start()
            lat_sends.append(c)

    sp_copies = []
    for d in range(1, n_sp):
        c = remote(
            part, parts.at[sp], sp_send.at[0, d - 1], sp_recv.at[0, d - 1],
            (lax.rem(sp + d, n_sp), tp),
        )
        c.start()
        sp_copies.append(c)
    send_piece(0)
    for piece in range(PIECES):
        c = row_copy(tp, piece, lat_send.at[0, piece], twin)
        c.start()
        lat_sends.append(c)
    parts[sp] = part[...]

    loads[3].wait()
    r = jnp.dot(act, w_mod[2], preferred_element_type=F32)
    for k in range(bands):
        part_g[k : k + 1, :] = r[0:1, k * 128 : (k + 1) * 128]
    parts_g[sp] = part_g[...]
    loads[-1].start()
    for d in range(chips):
        chip = lax.rem(x - d + chips, chips)
        lane = lax.broadcasted_iota(jnp.int32, (QUARTER, width), 1)
        if parts_in(d) > 1:
            lane = lane // step % 2 * own_rows + lane // part_width * step + lane % step
        place = sp * tok + chip * width + lane
        turn = lax.broadcasted_iota(jnp.int32, (QUARTER, width), 0).astype(F32)
        freq = jnp.exp(turn * (-math.log(rope_base) / QUARTER))
        by_row = (place // GRID_W).astype(F32) * freq
        by_col = (place % GRID_W).astype(F32) * freq
        table[d, 0:QUARTER, :] = jnp.cos(by_row)
        table[d, QUARTER : 2 * QUARTER, :] = jnp.sin(by_row)
        table[d, 2 * QUARTER : 3 * QUARTER, :] = jnp.cos(by_col)
        table[d, 3 * QUARTER :, :] = jnp.sin(by_col)
    k_pair = jnp.concatenate([k_gain[...], k_gain[...]], axis=1)
    for ref, dst in ((q_gain, gain_q), (k_gain, gain_k)):
        row = jnp.concatenate([ref[...], ref[...]], axis=1)
        square = jnp.transpose(jnp.broadcast_to(row, (128, 128)))[0:SPAN, :]
        for c in range(0, width, 128):
            dst[:, c : c + 128] = square
    peak[...] = jnp.full_like(peak, -1e30)
    acc[...] = jnp.zeros_like(acc)
    kv_all[:, 2 * SPAN :, :] = jnp.ones((kv_all.shape[0], 16, width), BF16)

    for c in sp_copies:
        c.wait()
    summed = parts[0]
    for j in range(1, n_sp):
        summed = summed + parts[j]
    part[...] = summed
    mods[tp] = summed
    tp_copies = []
    for d in range(1, n_tp):
        c = remote(
            part, mods.at[tp], tp_send.at[0, d - 1], tp_recv.at[0, d - 1],
            (sp, lax.rem(tp + d, n_tp)),
        )
        c.start()
        tp_copies.append(c)
    for piece in range(1, PIECES):
        send_piece(piece)
    gate_copies = []
    for d in range(1, n_sp):
        c = remote(
            part_g, parts_g.at[sp], sp_send.at[1, d - 1], sp_recv.at[1, d - 1],
            (lax.rem(sp + d, n_sp), tp),
        )
        c.start()
        gate_copies.append(c)
    for c in loads[4:-1]:
        c.wait()
    if kv_width % 128 != 0:
        w_all[:, q_width:] = jnp.concatenate([w_side[0], w_side[1]], axis=1)
    for piece in range(PIECES):
        row_copy(twin, piece, lat_send.at[0, 0], twin).wait_recv()
    for c in tp_copies:
        c.wait()
    for t in range(n_tp):
        for k in range(bands):
            cols = slice(t * columns + k * 128, t * columns + (k + 1) * 128)
            for row in range(2):
                at = (2 + row) * bands + k
                coef[row : row + 1, cols] = norm_gain[:, cols] * (1.0 + mods[t, at : at + 1, :])
                at = row * bands + k
                coef[2 + row : 3 + row, cols] = mods[t, at : at + 1, :]

    block = 16

    def modulate(read, rows, first, row):
        def body(i, carry):
            w = read(i * block).astype(F32)
            inv = lax.rsqrt(jnp.sum(w * w, axis=-1, keepdims=True) / model + epsilon)
            y = w * inv * coef[row : row + 1, :] + coef[2 + row : 3 + row, :]
            hidden[pl.ds(pl.multiple_of(first + i * block, block), block), :] = y.astype(BF16)
            return carry

        lax.fori_loop(0, rows // block, body, 0, unroll=min(4, rows // block))

    z_order = list(range(highs - 1, 0, -1))
    tail_sends = []

    def begin(c):
        c.start()
        tail_sends.append(c)

    def ctx_copy(head, src, ssem, z, y):
        return remote(ctx_send.at[head], ctx_all.at[src], ssem, c_recv.at[src], (dev(z, y), tp))

    def context_step():
        modulate(
            lambda i: context[pl.ds(pl.multiple_of(i, block), block), :], ctx_rows, 0, 1
        )
        raw = jnp.dot(hidden[0:ctx_rows, :], w_all[:, q_width:], preferred_element_type=F32)
        if groups == 2:
            k, val = raw[:, :kv_width], raw[:, kv_width:]
            first = lax.broadcasted_iota(jnp.int32, k.shape, 1) < SPAN
            sq = k * k
            s0 = jnp.sum(jnp.where(first, sq, 0.0), axis=-1, keepdims=True)
            s1 = jnp.sum(jnp.where(first, 0.0, sq), axis=-1, keepdims=True)
            scale = jnp.where(
                first, lax.rsqrt(s0 / SPAN + epsilon), lax.rsqrt(s1 / SPAN + epsilon)
            )
            k = k * scale * k_pair
            ctx_send[0] = jnp.where(first, k, pltpu.roll(val, SPAN, 1)).astype(BF16)
            ctx_send[1] = jnp.where(first, pltpu.roll(k, SPAN, 1), val).astype(BF16)
        else:
            first = lax.broadcasted_iota(jnp.int32, raw.shape, 1) < SPAN
            s0 = jnp.sum(jnp.where(first, raw * raw, 0.0), axis=-1, keepdims=True)
            k = raw * lax.rsqrt(s0 / SPAN + epsilon) * k_pair
            ctx_send[0] = jnp.where(first, k, raw).astype(BF16)
        for dz in z_order:
            z = lax.rem(high + dz, highs)
            begin(ctx_copy(lax.rem(z, groups), sp, cz_send.at[dz - 1], z, low))
        for dl in range(1, lows):
            begin(ctx_copy(g, sp, cy_send.at[dl - 1], high, lax.rem(low + dl, lows)))
        ctx_all[sp] = ctx_send[g]

    def finish(raw_head, gain, d, lanes):
        n = lanes.stop - lanes.start
        inv = lax.rsqrt(jnp.sum(raw_head * raw_head, axis=0, keepdims=True) / SPAN + epsilon)
        y = raw_head * inv * gain[:, 0:n]
        a1, b1 = y[0:QUARTER], y[QUARTER : 2 * QUARTER]
        a2, b2 = y[2 * QUARTER : 3 * QUARTER], y[3 * QUARTER :]
        cr, sr = table[d, 0:QUARTER, lanes], table[d, QUARTER : 2 * QUARTER, lanes]
        cc, sc = table[d, 2 * QUARTER : 3 * QUARTER, lanes], table[d, 3 * QUARTER :, lanes]
        return jnp.concatenate(
            [a1 * cr - b1 * sr, b1 * cr + a1 * sr, a2 * cc - b2 * sc, b2 * cc + a2 * sc], axis=0
        )

    def q_copy(d, p, group, ssem, z):
        lanes = lanes_of(d, p)
        return remote(
            q_send.at[d, group, :, :, lanes], q_raw.at[d, g, :, :, lanes], ssem,
            q_rsem.at[d, p, g], (dev(z, low), tp),
        )

    def q_store(d, group, value):
        f = value.astype(F32) * LOG2E
        hi = f.astype(BF16)
        q_all[d * groups + group, :, 0:SPAN, :] = hi
        q_all[d * groups + group, :, SPAN:, :] = (f - hi.astype(F32)).astype(BF16)

    def q_own(d):
        q_store(d, g, q_send[d, g])

    def q_arrive(d):
        for r in range(1, groups):
            other = lax.rem(g + r, groups)
            for p in range(parts_in(d)):
                lanes = lanes_of(d, p)
                dst = q_raw.at[d, other, :, :, lanes]
                remote(
                    dst, dst, q_ssem.at[d, 0, 0], q_rsem.at[d, p, other], (dev(base + other, low), tp)
                ).wait_recv()
            q_store(d, other, q_raw[d, other])

    def kv_copy(src_ref, d, p, src, ssem, z, y):
        lanes = lanes_of(d, p)
        return remote(
            src_ref, kv_all.at[d * n_sp + src, 0 : 2 * SPAN, lanes], ssem, kv_recv.at[d, p, src],
            (dev(z, y), tp),
        )

    def key_rows(slot, lanes):
        k = kv_all[slot, 0:SPAN, lanes]
        k_nat[slot, lanes, :] = jnp.transpose(jnp.concatenate([k, k], axis=0))

    def project(d, p):
        chip = lax.rem(x - d + chips, chips)
        lanes = lanes_of(d, p)
        n = lanes.stop - lanes.start
        if n == width:
            modulate(
                lambda i: lat[chip, pl.ds(pl.multiple_of(i, block), block), :], width, 0, 0
            )
        else:
            for half in range(2):
                at = half * own_rows + p * step
                modulate(
                    lambda i: lat[chip, pl.ds(pl.multiple_of(at + i, block), block), :],
                    step, half * step, 0,
                )
        flat = jnp.dot(hidden[0:n, :], w_all[...], preferred_element_type=F32)
        up = jnp.transpose(flat)
        for j in range(groups):
            r = q_width + j * SPAN
            kv_send[d, j, 0:SPAN, lanes] = finish(up[r : r + SPAN], gain_k, d, lanes).astype(BF16)
            r = q_width + kv_width + j * SPAN
            kv_send[d, j, SPAN:, lanes] = up[r : r + SPAN].astype(BF16)
            for h in range(heads):
                r = (j * heads + h) * SPAN
                y = finish(up[r : r + SPAN], gain_q, d, lanes)
                q_send[d, j, h, :, lanes] = (y * SPAN ** (-0.5)).astype(BF16)
        if d == 0:
            for r in range(1, groups):
                other = lax.rem(g + r, groups)
                begin(q_copy(d, p, other, q_ssem.at[d, p, r - 1], base + other))
        for dz in z_order:
            z = lax.rem(high + dz, highs)
            src = kv_send.at[d, lax.rem(z, groups), :, lanes]
            begin(kv_copy(src, d, p, sp, z_send.at[d, p, dz - 1], z, low))
        for dl in range(1, lows):
            y = lax.rem(low + dl, lows)
            src = kv_send.at[d, g, :, lanes]
            begin(kv_copy(src, d, p, sp, y_send.at[d, p, dl - 1], high, y))
        if d > 0:
            for r in range(1, groups):
                other = lax.rem(g + r, groups)
                begin(q_copy(d, p, other, q_ssem.at[d, p, r - 1], base + other))
        kv_all[d * n_sp + sp, 0 : 2 * SPAN, lanes] = kv_send[d, g, :, lanes]
        key_rows(d * n_sp + sp, lanes)

    def column(d, p, dz):
        src = dev(lax.rem(high - dz + highs, highs), low)
        slot = d * n_sp + src
        lanes = lanes_of(d, p)
        here = kv_all.at[slot, 0 : 2 * SPAN, lanes]
        kv_copy(here, d, p, src, z_send.at[0, 0, 0], high, low).wait_recv()
        for dl in range(1, lows):
            y = lax.rem(low + dl, lows)
            begin(kv_copy(here, d, p, src, f_send.at[d, p, dz - 1, dl - 1], high, y))
        key_rows(slot, lanes)

    def ctx_column(dz):
        src = dev(lax.rem(high - dz + highs, highs), low)
        ctx_copy(0, src, cz_send.at[0], high, low).wait_recv()
        for dl in range(1, lows):
            y = lax.rem(low + dl, lows)
            begin(
                remote(
                    ctx_all.at[src], ctx_all.at[src], cf_send.at[dz - 1, dl - 1],
                    c_recv.at[src], (dev(high, y), tp),
                )
            )

    def side(d, dz, dl):
        src = dev(lax.rem(high - dz + highs, highs), lax.rem(low - dl + lows, lows))
        slot = d * n_sp + src
        for p in range(parts_in(d)):
            lanes = lanes_of(d, p)
            here = kv_all.at[slot, 0 : 2 * SPAN, lanes]
            kv_copy(here, d, p, src, z_send.at[0, 0, 0], high, low).wait_recv()
            key_rows(slot, lanes)

    def ctx_ready():
        for dl in range(1, lows):
            for dz in range(highs):
                src = dev(lax.rem(high - dz + highs, highs), lax.rem(low - dl + lows, lows))
                ctx_copy(0, src, cz_send.at[0], high, low).wait_recv()
        per = width // ctx_rows
        for c in range(ctx_slots):
            piece = ctx_all[c * per : (c + 1) * per].reshape(width, 2 * SPAN)
            kv_all[ctx_first + c, 0 : 2 * SPAN, :] = jnp.transpose(piece)
            key_rows(ctx_first + c, slice(0, width))

    def slot_of(d, dz, dl):
        return d * n_sp + dev(
            lax.rem(high - dz + highs, highs), lax.rem(low - dl + lows, lows)
        )

    def run(steps):
        queue, owed = [], []

        def settle(limit):
            while len(owed) > limit:
                w, shrink, t, h, action = owed.pop(0)
                acc[t, h] = acc[t, h] * shrink + w
                if action is not None:
                    settle(0)
                    action()

        def soft():
            s, slot, t, h, action = queue.pop(0)
            old = peak[t, h, 0:1, :]
            top = jnp.maximum(jnp.max(s, axis=0, keepdims=True), old)
            shrink = jnp.exp2(old - top)
            e = jnp.exp2(s - top).astype(BF16)
            peak[t, h] = jnp.broadcast_to(top, (8, width))
            w = jnp.dot(kv_all[slot, SPAN:, :], e, preferred_element_type=F32)
            owed.append((w, shrink, t, h, action))
            settle(OWE)

        for kind, *rest in steps:
            if kind == "do":
                rest[0]()
                continue
            slot, t, action = rest
            for h in range(heads):
                r = jnp.dot(k_nat[slot], q_all[t, h], preferred_element_type=F32)
                if isinstance(slot, int) and slot >= ctx_first:
                    r = r + offset * LOG2E
                queue.append((r, slot, t, h, action if h == heads - 1 else None))
                if len(queue) > LAG:
                    soft()
        while queue:
            soft()
        settle(0)

    def attend(items):
        run([("at", s, t, None) for s, t in items])

    def attend_range(first, count, tile_list):
        per = math.gcd(max(1, 8 // len(tile_list)), count)

        def body(i, carry):
            attend([(first + i * per + u, t) for u in range(per) for t in tile_list])
            return carry

        lax.fori_loop(0, count // per, body, 0)

    def fetch(d, piece):
        chip = lax.rem(x - d + chips, chips)
        near = 2 * chip + core
        row_copy(near, piece, lat_send.at[0, 0], twin).wait_recv()
        begin(row_copy(near, piece, lat_fwd.at[d - 1, piece], twin))

    def fetch_back(d, piece):
        chip = lax.rem(x - d + chips, chips)
        row_copy(2 * chip + 1 - core, piece, lat_send.at[0, 0], twin).wait_recv()

    copies = []

    def deliver(d, r):
        chip = lax.rem(x - d + chips, chips)
        j = lax.rem(g + r, groups)
        t = d * groups + j
        rows = []
        for h in range(heads):
            inv = 1.0 / acc[t, h, SPAN : SPAN + 1, :]
            rows.append(acc[t, h, 0:SPAN, :] * inv)
        turned = jnp.transpose(jnp.concatenate(rows, axis=0)).astype(BF16)
        if parts_in(d) == 1:
            attended[d, r] = turned
        else:
            for p in range(split):
                for half in range(2):
                    at = half * own_rows + p * step
                    took = p * part_width + half * step
                    attended[d, r, at : at + step, :] = turned[took : took + step]
        for rc in range(2):
            half = lax.rem(core + rc, 2)
            src = attended.at[d, r, pl.ds(pl.multiple_of(half * own_rows, own_rows), own_rows), :]
            if d == 0 and r == 0 and rc == 0:
                received[tp * groups + g] = src[...]
            else:
                c = remote(
                    src, received.at[tp * groups + g], at_send.at[d, r, rc],
                    at_recv.at[tp * groups + g], (dev(base + j, low), 2 * chip + half),
                )
                c.start()
                copies.append(c)

    def gates():
        for c in gate_copies:
            c.wait()
        whole = parts_g[0]
        for j in range(1, n_sp):
            whole = whole + parts_g[j]
        part_g[...] = whole
        mods_g[tp] = whole
        result = []
        for d in range(1, n_tp):
            c = remote(
                part_g, mods_g.at[tp], tp_send.at[1, d - 1], tp_recv.at[1, d - 1],
                (sp, lax.rem(tp + d, n_tp)),
            )
            c.start()
            result.append(c)
        return result

    def tile_of(d, r):
        return d * groups + lax.rem(g + r, groups)

    if chips == 2 and split == 2 and n_sp == 8 and groups == 2:
        project(0, 0)
        fetch(1, 0)
        context_step()
        fetch_back(1, 0)
        project(1, 0)
        gate_out = gates()
        za, zb, zc = z_order
        own_a, mate_a, own_b, mate_b = (tile_of(d, r) for d in range(2) for r in range(2))
        early = [own_a, mate_a]
        ctx = range(ctx_first, ctx_first + ctx_slots)
        steps = []

        def do(action, *given):
            steps.append(("do", functools.partial(action, *given)))

        def at(slots, tiles):
            steps.extend(("at", s, t, None) for s in slots for t in tiles)

        q_own(0)
        q_arrive(0)
        at([slot_of(0, 0, 0)], early)
        do(side, 0, 0, 1)
        at([slot_of(0, 0, 1)], early)
        do(column, 0, 0, za)
        do(fetch, 1, 1)
        at([slot_of(0, za, 0)], early)
        do(column, 0, 0, zb)
        at([slot_of(0, zb, 0)], early)
        do(fetch_back, 1, 1)
        do(project, 1, 1)
        do(q_own, 1)
        do(column, 0, 0, zc)
        for dz in z_order:
            do(ctx_column, dz)
        most = early + [own_b]
        at([slot_of(0, zc, 0), slot_of(1, 0, 0)], most)
        at([slot_of(0, dz, 0) for dz in (0, za, zb)] + [slot_of(0, 0, 1)], [own_b])
        do(column, 1, 0, za)
        do(side, 0, za, 1)
        at([slot_of(0, za, 1)], most)
        do(column, 1, 0, zb)
        do(side, 0, zb, 1)
        at([slot_of(0, zb, 1)], most)
        do(ctx_ready)
        at(ctx, most)
        do(column, 1, 0, zc)
        do(side, 0, zc, 1)
        at([slot_of(0, zc, 1)], most)
        do(side, 1, 0, 1)
        at([slot_of(1, 0, 1)], most)
        do(column, 1, 1, za)
        at([slot_of(1, za, 0)], most)
        do(column, 1, 1, zb)
        do(q_arrive, 1)
        at(range(n_sp // 2), [mate_b])
        do(column, 1, 1, zc)
        at([slot_of(1, zb, 0), slot_of(1, zc, 0)], most)
        at(range(n_sp // 2, n_sp), [mate_b])
        at(ctx, [mate_b])
        at([slot_of(1, dz, 0) for dz in [0] + z_order] + [slot_of(1, 0, 1)], [mate_b])
        every = [mate_a, mate_b, own_b, own_a]
        do(side, 1, za, 1)
        at([slot_of(1, za, 1)], every)
        do(side, 1, zb, 1)
        do(side, 1, zc, 1)
        for place, t in zip(((0, 1), (1, 1), (1, 0), (0, 0)), every):
            at([slot_of(1, zb, 1)], [t])
            end = functools.partial(deliver, *place)
            steps.append(("at", slot_of(1, zc, 1), t, end))
        run(steps)
    else:
        context_step()
        for d in range(chips):
            if d > 0:
                for piece in range(PIECES):
                    fetch(d, piece)
                for piece in range(PIECES):
                    fetch_back(d, piece)
            for p in range(parts_in(d)):
                project(d, p)
            q_own(d)
        gate_out = gates()
        for dz in z_order:
            ctx_column(dz)
        for d in range(chips):
            for p in range(parts_in(d)):
                for dz in z_order:
                    column(d, p, dz)
            q_arrive(d)
        ctx_ready()
        for d in range(chips):
            for dl in range(1, lows):
                for dz in range(highs):
                    side(d, dz, dl)
        for d in range(chips):
            for r in range(groups):
                t = tile_of(d, r)
                attend_range(0, ctx_first, [t])
                attend([(s, t) for s in range(ctx_first, ctx_first + ctx_slots)])
                deliver(d, r)

    loads[-1].wait()
    for c in gate_out:
        c.wait()
    for rt in range(n_tp):
        for r in range(groups):
            if rt == 0 and r == 0:
                continue
            who = lax.rem(tp + rt, n_tp) * groups + lax.rem(g + r, groups)
            remote(
                received.at[who], received.at[who], at_send.at[0, 0, 1], at_recv.at[who],
                (sp, twin),
            ).wait_recv()
    rows = jnp.concatenate([received[s] for s in range(n_tp * groups)], axis=1)
    for t in range(n_tp):
        cols = slice(t * columns, (t + 1) * columns)
        gate = jnp.concatenate([mods_g[t, k : k + 1, :] for k in range(bands)], axis=1)
        branch = jnp.dot(rows, w_out[:, cols], preferred_element_type=F32)
        out[:, cols] = (lat[x, mine_rows, cols].astype(F32) + gate * branch).astype(BF16)
    for c in lat_sends + tail_sends + copies:
        c.wait_send()


def on_device(
    latent, context, condition, context_condition, norm_gain, shift_weight, scale_weight,
    gate_weight, query_weight, key_weight, value_weight, query_gain, key_gain, output_weight,
):
    n_sp, n_tp = lax.axis_size("sp"), lax.axis_size("tp")
    row_slab, columns = shift_weight.shape
    own_rows, model = latent.shape
    ctx_rows = context.shape[0]
    tok = own_rows * n_tp
    q_width, kv_width = query_weight.shape[1], key_weight.shape[1]
    groups = kv_width // SPAN
    heads = q_width // SPAN // groups
    chips = n_tp // 2
    width = 2 * own_rows
    lows = 2 ** (int(math.log2(n_sp)) // 2)
    highs = n_sp // lows
    slots = chips * n_sp + n_sp * ctx_rows // width
    n_tiles = chips * groups
    split = 2 if width // 2 % 128 == 0 else 1
    bands = columns // 128
    offset = math.log(tok / (2.0 * ctx_rows))
    dma = pltpu.SemaphoreType.DMA

    def stay(a):
        return pltpu.with_memory_space_constraint(a, pltpu.HBM)

    return pl.pallas_call(
        functools.partial(kernel, n_sp, n_tp, lows, offset, split),
        out_shape=jax.ShapeDtypeStruct(latent.shape, BF16),
        in_specs=[ANY] * 14,
        out_specs=VMEM,
        scratch_shapes=[
            pltpu.VMEM((1, model), F32), pltpu.VMEM((1, model), F32), pltpu.VMEM((1, model), F32),
            pltpu.VMEM((1, SPAN), F32), pltpu.VMEM((1, SPAN), F32),
            pltpu.VMEM((chips, width, model), BF16),
            pltpu.VMEM(context.shape, BF16),
            pltpu.VMEM((3, row_slab, columns), BF16),
            pltpu.VMEM((model, q_width + 2 * kv_width), BF16),
            pltpu.VMEM((2,) + (key_weight.shape if kv_width % 128 else (16, 128)), BF16),
            pltpu.VMEM(output_weight.shape, BF16),
            pltpu.VMEM((4 * bands, 128), F32),
            pltpu.VMEM((n_sp, 4 * bands, 128), F32),
            pltpu.VMEM((n_tp, 4 * bands, 128), F32),
            pltpu.VMEM((8, 128), F32),
            pltpu.VMEM((n_sp, 8, 128), F32),
            pltpu.VMEM((n_tp, 8, 128), F32),
            pltpu.VMEM((8, model), F32),
            pltpu.VMEM((width, model), BF16),
            pltpu.VMEM((chips, SPAN, width), F32),
            pltpu.VMEM((SPAN, width), F32),
            pltpu.VMEM((SPAN, width), F32),
            pltpu.VMEM((chips, groups, heads, SPAN, width), BF16),
            pltpu.VMEM((chips, groups, heads, SPAN, width), BF16),
            pltpu.VMEM((chips, groups, 2 * SPAN, width), BF16),
            pltpu.VMEM((groups, ctx_rows, 2 * SPAN), BF16),
            pltpu.VMEM((n_sp, ctx_rows, 2 * SPAN), BF16),
            pltpu.VMEM((n_tiles, heads, 2 * SPAN, width), BF16),
            pltpu.VMEM((slots, 2 * SPAN + 16, width), BF16),
            pltpu.VMEM((slots, width, 2 * SPAN), BF16),
            pltpu.VMEM((n_tiles, heads, 8, width), F32),
            pltpu.VMEM((n_tiles, heads, SPAN + 16, width), F32),
            pltpu.VMEM((chips, groups, width, 2 * SPAN), BF16),
            pltpu.VMEM((n_tp * groups, own_rows, 2 * SPAN), BF16),
            dma((9,)), dma((chips, PIECES)), dma((max(chips - 1, 1), PIECES)), dma((n_tp, PIECES)),
            dma((2, n_sp - 1)), dma((2, n_sp - 1)), dma((2, n_tp - 1)), dma((2, n_tp - 1)),
            dma((chips, split, max(groups - 1, 1))), dma((chips, split, groups)),
            dma((chips, split, highs - 1)), dma((chips, split, lows - 1)),
            dma((chips, split, highs - 1, lows - 1)), dma((chips, split, n_sp)),
            dma((highs - 1,)), dma((lows - 1,)), dma((highs - 1, lows - 1)), dma((n_sp,)),
            dma((chips, groups, 2)), dma((n_tp * groups,)), dma((5,)),
        ],
        compiler_params=pltpu.CompilerParams(
            collective_id=0, has_side_effects=True, vmem_limit_bytes=46 << 20
        ),
        name="fused",
    )(
        stay(latent), stay(context), stay(condition[None]), stay(context_condition[None]),
        stay(norm_gain[None]),
        stay(shift_weight), stay(scale_weight), stay(gate_weight), stay(query_weight),
        stay(key_weight), stay(value_weight), stay(query_gain[None]), stay(key_gain[None]),
        stay(output_weight),
    )


def solution(mesh):
    in_specs = (
        P(("sp", "tp"), None), P("sp", None), P(), P(), P(),
        P("sp", "tp"), P("sp", "tp"), P("sp", "tp"),
        P(None, "tp"), P(None, "tp"), P(None, "tp"), P(), P(), P(),
    )
    return jax.shard_map(
        on_device, mesh=mesh, in_specs=in_specs, out_specs=P(("sp", "tp"), None), check_vma=False
    )
```

```python
import functools
import math

import jax
import jax.numpy as jnp
from jax import lax
from jax.experimental import pallas as pl
from jax.experimental.pallas import tpu as pltpu
from jax.sharding import PartitionSpec as P

SPAN = 64
GRID_W = 64
QUARTER = SPAN // 4
LAG = 5
OWE = 0
PIECES = 2
LOG2E = 1.4426950408889634
MESH = pl.DeviceIdType.MESH
VMEM = pl.BlockSpec(memory_space=pltpu.VMEM)
ANY = pl.BlockSpec(memory_space=pl.ANY)
F32 = jnp.float32
BF16 = jnp.bfloat16

epsilon = 1e-06
rope_base = 10000.0


def kernel(
    n_sp, n_tp, lows, offset, split,
    latent_hbm, context_hbm, cond_hbm, ctx_cond_hbm, norm_gain_hbm, w_shift_hbm, w_scale_hbm,
    w_gate_hbm, w_q_hbm, w_k_hbm, w_v_hbm, q_gain_hbm, k_gain_hbm, w_out_hbm,
    out, cond, ctx_cond, norm_gain, q_gain, k_gain,
    lat, context, w_mod, w_all, w_side, w_out, part, parts, mods, part_g, parts_g, mods_g,
    coef, hidden, table, gain_q, gain_k, q_send, q_raw, kv_send, ctx_send, ctx_all, q_all, kv_all,
    k_nat, peak, acc, attended, received,
    load, lat_send, lat_fwd, lat_recv, sp_send, sp_recv, tp_send, tp_recv,
    q_ssem, q_rsem, z_send, y_send, f_send, kv_recv,
    cz_send, cy_send, cf_send, c_recv, at_send, at_recv, small_sem, summed_out, inverse,
):
    sp, tp = lax.axis_index("sp"), lax.axis_index("tp")
    chips = n_tp // 2
    highs = n_sp // lows
    low, high = lax.rem(sp, lows), sp // lows
    x, core = tp // 2, lax.rem(tp, 2)
    twin = tp + 1 - 2 * core
    width = lat.shape[1]
    own_rows = width // 2
    model = lat.shape[2]
    tok = chips * width
    ctx_rows = context.shape[0]
    groups = kv_send.shape[1]
    heads = q_send.shape[2]
    q_width = groups * heads * SPAN
    kv_width = groups * SPAN
    row_slab, columns = w_mod.shape[1], w_mod.shape[2]
    bands = columns // 128
    g = lax.rem(high, groups)
    base = high - g
    ctx_slots = n_sp * ctx_rows // width
    ctx_first = chips * n_sp
    step = own_rows // PIECES
    part_width = width // split

    def dev(z, y):
        return z * lows + y

    def remote(src, dst, ssem, rsem, peer):
        return pltpu.make_async_remote_copy(
            src_ref=src, dst_ref=dst, send_sem=ssem, recv_sem=rsem,
            device_id=peer, device_id_type=MESH,
        )

    def lanes_of(d, p):
        if d == 0 or split == 1:
            return slice(0, width)
        return slice(p * part_width, (p + 1) * part_width)

    def parts_in(d):
        return 1 if d == 0 else split

    barrier = pltpu.get_barrier_semaphore()
    peers = [(lax.rem(sp + d, n_sp), tp) for d in range(1, n_sp)]
    peers += [(sp, lax.rem(tp + d, n_tp)) for d in range(1, n_tp)]
    for r in range(1, groups):
        mate = dev(base + lax.rem(g + r, groups), low)
        peers += [(mate, lax.rem(tp + d, n_tp)) for d in range(1, n_tp)]
    for p in peers:
        pl.semaphore_signal(barrier, inc=1, device_id=p, device_id_type=MESH)

    mine_rows = pl.ds(pl.multiple_of(core * own_rows, own_rows), own_rows)
    pairs = [
        (w_shift_hbm, w_mod.at[0]), (w_scale_hbm, w_mod.at[1]),
        (latent_hbm, lat.at[x, mine_rows, :]), (w_gate_hbm, w_mod.at[2]),
        (context_hbm, context), (w_q_hbm, w_all.at[:, 0:q_width]),
    ]
    if kv_width % 128 == 0:
        pairs += [
            (w_k_hbm, w_all.at[:, q_width : q_width + kv_width]),
            (w_v_hbm, w_all.at[:, q_width + kv_width :]),
        ]
    else:
        pairs += [(w_k_hbm, w_side.at[0]), (w_v_hbm, w_side.at[1])]
    pairs.append((w_out_hbm, w_out))
    small = [
        pltpu.make_async_copy(s, d, small_sem.at[i])
        for i, (s, d) in enumerate(
            (
                (cond_hbm, cond), (ctx_cond_hbm, ctx_cond), (norm_gain_hbm, norm_gain),
                (q_gain_hbm, q_gain), (k_gain_hbm, k_gain),
            )
        )
    ]
    for c in small:
        c.start()
    loads = [pltpu.make_async_copy(s, d, load.at[i]) for i, (s, d) in enumerate(pairs)]
    for c in loads[:-1]:
        c.start()

    def slab(ref):
        if row_slab % 128 == 0:
            return ref[:, pl.ds(pl.multiple_of(sp * row_slab, 128), row_slab)]
        per = 128 // row_slab
        window = ref[:, pl.ds(pl.multiple_of(sp // per * 128, 128), 128)]
        pick = lax.rem(sp, per)
        result = window
        for k in range(1, per):
            result = jnp.where(pick == k, pltpu.roll(window, 128 - k * row_slab, 1), result)
        return result[:, :row_slab]

    for c in small:
        c.wait()
    v = jnp.concatenate([slab(cond), slab(ctx_cond)], axis=0)
    act = (v / (1.0 + jnp.exp(-v))).astype(BF16)
    part_g[...] = jnp.zeros_like(part_g)
    for i in range(2):
        loads[i].wait()
        r = jnp.dot(act, w_mod[i], preferred_element_type=F32)
        for row in range(2):
            for k in range(bands):
                at = (2 * i + row) * bands + k
                part[at : at + 1, :] = r[row : row + 1, k * 128 : (k + 1) * 128]
    loads[2].wait()
    pl.semaphore_wait(barrier, len(peers))

    def rows_of(tile, piece):
        chip, half = tile // 2, lax.rem(tile, 2)
        start = pl.multiple_of(half * own_rows + piece * step, step)
        return lat.at[chip, pl.ds(start, step), :]

    def row_copy(tile, piece, ssem, peer):
        return remote(
            rows_of(tile, piece), rows_of(tile, piece), ssem, lat_recv.at[tile, piece], (sp, peer)
        )

    lat_sends = []

    def send_piece(piece):
        for d in range(1, chips):
            c = row_copy(tp, piece, lat_send.at[d, piece], lax.rem(tp + 2 * d, n_tp))
            c.start()
            lat_sends.append(c)

    sp_copies = []
    for d in range(1, n_sp):
        c = remote(
            part, parts.at[sp], sp_send.at[0, d - 1], sp_recv.at[0, d - 1],
            (lax.rem(sp + d, n_sp), tp),
        )
        c.start()
        sp_copies.append(c)
    send_piece(0)
    for piece in range(PIECES):
        c = row_copy(tp, piece, lat_send.at[0, piece], twin)
        c.start()
        lat_sends.append(c)
    parts[sp] = part[...]

    loads[3].wait()
    r = jnp.dot(act, w_mod[2], preferred_element_type=F32)
    for k in range(bands):
        part_g[k : k + 1, :] = r[0:1, k * 128 : (k + 1) * 128]
    parts_g[sp] = part_g[...]
    loads[-1].start()
    for d in range(chips):
        chip = lax.rem(x - d + chips, chips)
        lane = lax.broadcasted_iota(jnp.int32, (QUARTER, width), 1)
        if parts_in(d) > 1:
            lane = lane // step % 2 * own_rows + lane // part_width * step + lane % step
        place = sp * tok + chip * width + lane
        turn = lax.broadcasted_iota(jnp.int32, (QUARTER, width), 0).astype(F32)
        freq = jnp.exp(turn * (-math.log(rope_base) / QUARTER))
        by_row = (place // GRID_W).astype(F32) * freq
        by_col = (place % GRID_W).astype(F32) * freq
        table[d, 0:QUARTER, :] = jnp.cos(by_row)
        table[d, QUARTER : 2 * QUARTER, :] = jnp.sin(by_row)
        table[d, 2 * QUARTER : 3 * QUARTER, :] = jnp.cos(by_col)
        table[d, 3 * QUARTER :, :] = jnp.sin(by_col)
    k_pair = jnp.concatenate([k_gain[...], k_gain[...]], axis=1)
    for ref, dst in ((q_gain, gain_q), (k_gain, gain_k)):
        row = jnp.concatenate([ref[...], ref[...]], axis=1)
        square = jnp.transpose(jnp.broadcast_to(row, (128, 128)))[0:SPAN, :]
        for c in range(0, width, 128):
            dst[:, c : c + 128] = square
    peak[...] = jnp.full_like(peak, -1e30)
    acc[...] = jnp.zeros_like(acc)
    kv_all[:, 2 * SPAN :, :] = jnp.ones((kv_all.shape[0], 16, width), BF16)

    for c in sp_copies:
        c.wait()
    summed = parts[0]
    for j in range(1, n_sp):
        summed = summed + parts[j]
    part[...] = summed
    mods[tp] = summed
    tp_copies = []
    for d in range(1, n_tp):
        c = remote(
            part, mods.at[tp], tp_send.at[0, d - 1], tp_recv.at[0, d - 1],
            (sp, lax.rem(tp + d, n_tp)),
        )
        c.start()
        tp_copies.append(c)
    for piece in range(1, PIECES):
        send_piece(piece)
    gate_copies = []
    for d in range(1, n_sp):
        c = remote(
            part_g, parts_g.at[sp], sp_send.at[1, d - 1], sp_recv.at[1, d - 1],
            (lax.rem(sp + d, n_sp), tp),
        )
        c.start()
        gate_copies.append(c)
    for c in loads[4:-1]:
        c.wait()
    if kv_width % 128 != 0:
        w_all[:, q_width:] = jnp.concatenate([w_side[0], w_side[1]], axis=1)
    for piece in range(PIECES):
        row_copy(twin, piece, lat_send.at[0, 0], twin).wait_recv()

    def measure(i, carry):
        r = pl.ds(pl.multiple_of(i * 16, 16), 16)
        w = lat[x, r, :].astype(F32)
        inv = lax.rsqrt(jnp.sum(w * w, axis=-1, keepdims=True) / model + epsilon)
        inverse[r, :] = jnp.broadcast_to(inv, (16, 128))
        return carry

    lax.fori_loop(0, width // 16, measure, 0, unroll=4)
    for c in tp_copies:
        c.wait()
    for t in range(n_tp):
        for k in range(bands):
            cols = slice(t * columns + k * 128, t * columns + (k + 1) * 128)
            for row in range(2):
                at = (2 + row) * bands + k
                coef[row : row + 1, cols] = norm_gain[:, cols] * (1.0 + mods[t, at : at + 1, :])
                at = row * bands + k
                coef[2 + row : 3 + row, cols] = mods[t, at : at + 1, :]

    block = 16

    def modulate(read, rows, first, row, known=False):
        def body(i, carry):
            w = read(i * block).astype(F32)
            if known:
                r = pl.ds(pl.multiple_of(i * block, block), block)
                inv = jnp.concatenate([inverse[r, :]] * (model // 128), axis=1)
            else:
                inv = lax.rsqrt(jnp.sum(w * w, axis=-1, keepdims=True) / model + epsilon)
            y = w * inv * coef[row : row + 1, :] + coef[2 + row : 3 + row, :]
            hidden[pl.ds(pl.multiple_of(first + i * block, block), block), :] = y.astype(BF16)
            return carry

        lax.fori_loop(0, rows // block, body, 0, unroll=min(4, rows // block))

    z_order = [d for d in range(1, highs)]
    z_order = z_order[1:2] + z_order[:1] + z_order[2:]
    tail_sends = []

    def begin(c):
        c.start()
        tail_sends.append(c)

    def ctx_copy(head, src, ssem, z, y):
        return remote(ctx_send.at[head], ctx_all.at[src], ssem, c_recv.at[src], (dev(z, y), tp))

    def context_step():
        modulate(
            lambda i: context[pl.ds(pl.multiple_of(i, block), block), :], ctx_rows, 0, 1
        )
        raw = jnp.dot(hidden[0:ctx_rows, :], w_all[:, q_width:], preferred_element_type=F32)
        if groups == 2:
            k, val = raw[:, :kv_width], raw[:, kv_width:]
            first = lax.broadcasted_iota(jnp.int32, k.shape, 1) < SPAN
            sq = k * k
            s0 = jnp.sum(jnp.where(first, sq, 0.0), axis=-1, keepdims=True)
            s1 = jnp.sum(jnp.where(first, 0.0, sq), axis=-1, keepdims=True)
            scale = jnp.where(
                first, lax.rsqrt(s0 / SPAN + epsilon), lax.rsqrt(s1 / SPAN + epsilon)
            )
            k = k * scale * k_pair
            ctx_send[0] = jnp.where(first, k, pltpu.roll(val, SPAN, 1)).astype(BF16)
            ctx_send[1] = jnp.where(first, pltpu.roll(k, SPAN, 1), val).astype(BF16)
        else:
            first = lax.broadcasted_iota(jnp.int32, raw.shape, 1) < SPAN
            s0 = jnp.sum(jnp.where(first, raw * raw, 0.0), axis=-1, keepdims=True)
            k = raw * lax.rsqrt(s0 / SPAN + epsilon) * k_pair
            ctx_send[0] = jnp.where(first, k, raw).astype(BF16)
        for dz in z_order:
            z = lax.rem(high + dz, highs)
            begin(ctx_copy(lax.rem(z, groups), sp, cz_send.at[dz - 1], z, low))
        for dl in range(1, lows):
            begin(ctx_copy(g, sp, cy_send.at[dl - 1], high, lax.rem(low + dl, lows)))
        ctx_all[sp] = ctx_send[g]

    def finish(raw_head, gain, d, lanes):
        n = lanes.stop - lanes.start
        inv = lax.rsqrt(jnp.sum(raw_head * raw_head, axis=0, keepdims=True) / SPAN + epsilon)
        y = raw_head * inv * gain[:, 0:n]
        a1, b1 = y[0:QUARTER], y[QUARTER : 2 * QUARTER]
        a2, b2 = y[2 * QUARTER : 3 * QUARTER], y[3 * QUARTER :]
        cr, sr = table[d, 0:QUARTER, lanes], table[d, QUARTER : 2 * QUARTER, lanes]
        cc, sc = table[d, 2 * QUARTER : 3 * QUARTER, lanes], table[d, 3 * QUARTER :, lanes]
        return jnp.concatenate(
            [a1 * cr - b1 * sr, b1 * cr + a1 * sr, a2 * cc - b2 * sc, b2 * cc + a2 * sc], axis=0
        )

    def q_copy(d, p, group, ssem, z):
        lanes = lanes_of(d, p)
        return remote(
            q_send.at[d, group, :, :, lanes], q_raw.at[d, g, :, :, lanes], ssem,
            q_rsem.at[d, p, g], (dev(z, low), tp),
        )

    def q_store(d, group, value):
        f = value.astype(F32) * LOG2E
        hi = f.astype(BF16)
        q_all[d * groups + group, :, 0:SPAN, :] = hi
        q_all[d * groups + group, :, SPAN:, :] = (f - hi.astype(F32)).astype(BF16)

    def q_own(d):
        q_store(d, g, q_send[d, g])

    def q_arrive(d):
        for r in range(1, groups):
            other = lax.rem(g + r, groups)
            for p in range(parts_in(d)):
                lanes = lanes_of(d, p)
                dst = q_raw.at[d, other, :, :, lanes]
                remote(
                    dst, dst, q_ssem.at[d, 0, 0], q_rsem.at[d, p, other], (dev(base + other, low), tp)
                ).wait_recv()
            q_store(d, other, q_raw[d, other])

    def kv_copy(src_ref, d, p, src, ssem, z, y):
        lanes = lanes_of(d, p)
        return remote(
            src_ref, kv_all.at[d * n_sp + src, 0 : 2 * SPAN, lanes], ssem, kv_recv.at[d, p, src],
            (dev(z, y), tp),
        )

    def key_rows(slot, lanes):
        k = kv_all[slot, 0:SPAN, lanes]
        k_nat[slot, lanes, :] = jnp.transpose(jnp.concatenate([k, k], axis=0))

    def project(d, p):
        chip = lax.rem(x - d + chips, chips)
        lanes = lanes_of(d, p)
        n = lanes.stop - lanes.start
        if n == width:
            modulate(
                lambda i: lat[chip, pl.ds(pl.multiple_of(i, block), block), :], width, 0, 0, d == 0
            )
        else:
            for half in range(2):
                at = half * own_rows + p * step
                modulate(
                    lambda i: lat[chip, pl.ds(pl.multiple_of(at + i, block), block), :],
                    step, half * step, 0,
                )
        flat = jnp.dot(hidden[0:n, :], w_all[...], preferred_element_type=F32)
        up = jnp.transpose(flat)
        for j in range(groups):
            r = q_width + j * SPAN
            kv_send[d, j, 0:SPAN, lanes] = finish(up[r : r + SPAN], gain_k, d, lanes).astype(BF16)
            r = q_width + kv_width + j * SPAN
            kv_send[d, j, SPAN:, lanes] = up[r : r + SPAN].astype(BF16)
            for h in range(heads):
                r = (j * heads + h) * SPAN
                y = finish(up[r : r + SPAN], gain_q, d, lanes)
                q_send[d, j, h, :, lanes] = (y * SPAN ** (-0.5)).astype(BF16)
        if d == 0:
            for r in range(1, groups):
                other = lax.rem(g + r, groups)
                begin(q_copy(d, p, other, q_ssem.at[d, p, r - 1], base + other))
        for dz in z_order:
            z = lax.rem(high + dz, highs)
            src = kv_send.at[d, lax.rem(z, groups), :, lanes]
            begin(kv_copy(src, d, p, sp, z_send.at[d, p, dz - 1], z, low))
        for dl in range(1, lows):
            y = lax.rem(low + dl, lows)
            src = kv_send.at[d, g, :, lanes]
            begin(kv_copy(src, d, p, sp, y_send.at[d, p, dl - 1], high, y))
        if d > 0:
            for r in range(1, groups):
                other = lax.rem(g + r, groups)
                begin(q_copy(d, p, other, q_ssem.at[d, p, r - 1], base + other))
        kv_all[d * n_sp + sp, 0 : 2 * SPAN, lanes] = kv_send[d, g, :, lanes]
        key_rows(d * n_sp + sp, lanes)

    def column(d, p, dz):
        src = dev(lax.rem(high - dz + highs, highs), low)
        slot = d * n_sp + src
        lanes = lanes_of(d, p)
        here = kv_all.at[slot, 0 : 2 * SPAN, lanes]
        kv_copy(here, d, p, src, z_send.at[0, 0, 0], high, low).wait_recv()
        for dl in range(1, lows):
            y = lax.rem(low + dl, lows)
            begin(kv_copy(here, d, p, src, f_send.at[d, p, dz - 1, dl - 1], high, y))
        key_rows(slot, lanes)

    def ctx_column(dz):
        src = dev(lax.rem(high - dz + highs, highs), low)
        ctx_copy(0, src, cz_send.at[0], high, low).wait_recv()
        for dl in range(1, lows):
            y = lax.rem(low + dl, lows)
            begin(
                remote(
                    ctx_all.at[src], ctx_all.at[src], cf_send.at[dz - 1, dl - 1],
                    c_recv.at[src], (dev(high, y), tp),
                )
            )

    def side(d, dz, dl):
        src = dev(lax.rem(high - dz + highs, highs), lax.rem(low - dl + lows, lows))
        slot = d * n_sp + src
        for p in range(parts_in(d)):
            lanes = lanes_of(d, p)
            here = kv_all.at[slot, 0 : 2 * SPAN, lanes]
            kv_copy(here, d, p, src, z_send.at[0, 0, 0], high, low).wait_recv()
            key_rows(slot, lanes)

    def ctx_ready():
        for dl in range(1, lows):
            for dz in range(highs):
                src = dev(lax.rem(high - dz + highs, highs), lax.rem(low - dl + lows, lows))
                ctx_copy(0, src, cz_send.at[0], high, low).wait_recv()
        per = width // ctx_rows
        for c in range(ctx_slots):
            piece = ctx_all[c * per : (c + 1) * per].reshape(width, 2 * SPAN)
            kv_all[ctx_first + c, 0 : 2 * SPAN, :] = jnp.transpose(piece)
            key_rows(ctx_first + c, slice(0, width))

    def slot_of(d, dz, dl):
        return d * n_sp + dev(
            lax.rem(high - dz + highs, highs), lax.rem(low - dl + lows, lows)
        )

    def run(steps):
        queue, owed = [], []

        def settle(limit):
            while len(owed) > limit:
                w, shrink, t, h, action = owed.pop(0)
                acc[t, h] = acc[t, h] * shrink + w
                if action is not None:
                    settle(0)
                    action()

        def soft():
            s, slot, t, h, action = queue.pop(0)
            old = peak[t, h, 0:1, :]
            top = jnp.maximum(jnp.max(s, axis=0, keepdims=True), old)
            shrink = jnp.exp2(old - top)
            e = jnp.exp2(s - top).astype(BF16)
            peak[t, h] = jnp.broadcast_to(top, (8, width))
            w = jnp.dot(kv_all[slot, SPAN:, :], e, preferred_element_type=F32)
            owed.append((w, shrink, t, h, action))
            settle(OWE)

        for kind, *rest in steps:
            if kind == "do":
                rest[0]()
                continue
            slot, t, action = rest
            for h in range(heads):
                r = jnp.dot(k_nat[slot], q_all[t, h], preferred_element_type=F32)
                if isinstance(slot, int) and slot >= ctx_first:
                    r = r + offset * LOG2E
                queue.append((r, slot, t, h, action if h == heads - 1 else None))
                if len(queue) > LAG:
                    soft()
        while queue:
            soft()
        settle(0)

    def attend(items):
        run([("at", s, t, None) for s, t in items])

    def attend_range(first, count, tile_list):
        per = math.gcd(max(1, 8 // len(tile_list)), count)

        def body(i, carry):
            attend([(first + i * per + u, t) for u in range(per) for t in tile_list])
            return carry

        lax.fori_loop(0, count // per, body, 0)

    def fetch(d, piece):
        chip = lax.rem(x - d + chips, chips)
        near = 2 * chip + core
        row_copy(near, piece, lat_send.at[0, 0], twin).wait_recv()
        begin(row_copy(near, piece, lat_fwd.at[d - 1, piece], twin))

    def fetch_back(d, piece):
        chip = lax.rem(x - d + chips, chips)
        row_copy(2 * chip + 1 - core, piece, lat_send.at[0, 0], twin).wait_recv()

    copies = []

    def deliver(d, r):
        chip = lax.rem(x - d + chips, chips)
        j = lax.rem(g + r, groups)
        t = d * groups + j
        rows = []
        for h in range(heads):
            inv = 1.0 / acc[t, h, SPAN : SPAN + 1, :]
            rows.append(acc[t, h, 0:SPAN, :] * inv)
        turned = jnp.transpose(jnp.concatenate(rows, axis=0)).astype(BF16)
        if parts_in(d) == 1:
            attended[d, r] = turned
        else:
            for p in range(split):
                for half in range(2):
                    at = half * own_rows + p * step
                    took = p * part_width + half * step
                    attended[d, r, at : at + step, :] = turned[took : took + step]
        for rc in range(2):
            half = lax.rem(core + rc, 2)
            src = attended.at[d, r, pl.ds(pl.multiple_of(half * own_rows, own_rows), own_rows), :]
            if d == 0 and r == 0 and rc == 0:
                received[tp * groups + g] = src[...]
            else:
                c = remote(
                    src, received.at[tp * groups + g], at_send.at[d, r, rc],
                    at_recv.at[tp * groups + g], (dev(base + j, low), 2 * chip + half),
                )
                c.start()
                copies.append(c)

    def gates():
        for c in gate_copies:
            c.wait()
        whole = parts_g[0]
        for j in range(1, n_sp):
            whole = whole + parts_g[j]
        part_g[...] = whole
        mods_g[tp] = whole
        result = []
        for d in range(1, n_tp):
            c = remote(
                part_g, mods_g.at[tp], tp_send.at[1, d - 1], tp_recv.at[1, d - 1],
                (sp, lax.rem(tp + d, n_tp)),
            )
            c.start()
            result.append(c)
        return result

    def tile_of(d, r):
        return d * groups + lax.rem(g + r, groups)

    if chips == 2 and split == 2 and n_sp == 8 and groups == 2:
        project(0, 0)
        fetch(1, 0)
        context_step()
        fetch_back(1, 0)
        project(1, 0)
        gate_out = gates()
        za, zb, zc = z_order
        own_a, mate_a, own_b, mate_b = (tile_of(d, r) for d in range(2) for r in range(2))
        early = [own_a, mate_a]
        ctx = range(ctx_first, ctx_first + ctx_slots)
        steps = []

        def do(action, *given):
            steps.append(("do", functools.partial(action, *given)))

        def at(slots, tiles):
            steps.extend(("at", s, t, None) for s in slots for t in tiles)

        q_own(0)
        q_arrive(0)
        at([slot_of(0, 0, 0)], early)
        do(side, 0, 0, 1)
        at([slot_of(0, 0, 1)], early)
        do(column, 0, 0, za)
        do(fetch, 1, 1)
        at([slot_of(0, za, 0)], early)
        do(column, 0, 0, zb)
        at([slot_of(0, zb, 0)], early)
        do(fetch_back, 1, 1)
        do(project, 1, 1)
        do(q_own, 1)
        do(column, 0, 0, zc)
        for dz in z_order:
            do(ctx_column, dz)
        most = early + [own_b]
        at([slot_of(0, zc, 0), slot_of(1, 0, 0)], most)
        at([slot_of(0, dz, 0) for dz in (0, za, zb)] + [slot_of(0, 0, 1)], [own_b])
        do(column, 1, 0, za)
        do(side, 0, za, 1)
        at([slot_of(0, za, 1)], most)
        do(column, 1, 0, zb)
        do(side, 0, zb, 1)
        at([slot_of(0, zb, 1)], most)
        do(ctx_ready)
        at(ctx, most)
        do(column, 1, 0, zc)
        do(side, 0, zc, 1)
        at([slot_of(0, zc, 1)], most)
        do(side, 1, 0, 1)
        at([slot_of(1, 0, 1)], most)
        do(column, 1, 1, za)
        at([slot_of(1, za, 0)], most)
        do(column, 1, 1, zb)
        at([slot_of(1, zb, 0)], most)
        do(column, 1, 1, zc)
        do(q_arrive, 1)
        at(range(n_sp), [mate_b])
        at(ctx, [mate_b])
        at([slot_of(1, zc, 0)], most)
        at([slot_of(1, dz, 0) for dz in [0] + z_order] + [slot_of(1, 0, 1)], [mate_b])
        every = [mate_a, mate_b, own_b, own_a]
        do(side, 1, za, 1)
        at([slot_of(1, za, 1)], every)
        do(side, 1, zb, 1)
        do(side, 1, zc, 1)
        for place, t in zip(((0, 1), (1, 1), (1, 0), (0, 0)), every):
            at([slot_of(1, zb, 1)], [t])
            end = functools.partial(deliver, *place)
            steps.append(("at", slot_of(1, zc, 1), t, end))
        run(steps)
    else:
        context_step()
        for d in range(chips):
            if d > 0:
                for piece in range(PIECES):
                    fetch(d, piece)
                for piece in range(PIECES):
                    fetch_back(d, piece)
            for p in range(parts_in(d)):
                project(d, p)
            q_own(d)
        gate_out = gates()
        for dz in z_order:
            ctx_column(dz)
        for d in range(chips):
            for p in range(parts_in(d)):
                for dz in z_order:
                    column(d, p, dz)
            q_arrive(d)
        ctx_ready()
        for d in range(chips):
            for dl in range(1, lows):
                for dz in range(highs):
                    side(d, dz, dl)
        for d in range(chips):
            for r in range(groups):
                t = tile_of(d, r)
                attend_range(0, ctx_first, [t])
                attend([(s, t) for s in range(ctx_first, ctx_first + ctx_slots)])
                deliver(d, r)

    loads[-1].wait()
    for c in gate_out:
        c.wait()
    order = [tp, twin]
    for d in range(1, chips):
        order += [lax.rem(tp + 2 * d, n_tp), lax.rem(twin + 2 * d, n_tp)]
    for n, src in enumerate(order):
        for r in range(groups):
            if n == 0 and r == 0:
                continue
            who = src * groups + lax.rem(g + r, groups)
            remote(
                received.at[who], received.at[who], at_send.at[0, 0, 1], at_recv.at[who],
                (sp, twin),
            ).wait_recv()
        depth = groups * 2 * SPAN
        rows = jnp.concatenate([received[src * groups + j] for j in range(groups)], axis=1)
        heights = pl.ds(pl.multiple_of(src * depth, depth), depth)
        for t in range(n_tp):
            cols = slice(t * columns, (t + 1) * columns)
            branch = jnp.dot(rows, w_out[heights, cols], preferred_element_type=F32)
            if n > 0:
                branch = branch + summed_out[:, cols]
            if n < len(order) - 1:
                summed_out[:, cols] = branch
            else:
                gate = jnp.concatenate([mods_g[t, k : k + 1, :] for k in range(bands)], axis=1)
                out[:, cols] = (lat[x, mine_rows, cols].astype(F32) + gate * branch).astype(BF16)
    for c in lat_sends + tail_sends + copies:
        c.wait_send()


def on_device(
    latent, context, condition, context_condition, norm_gain, shift_weight, scale_weight,
    gate_weight, query_weight, key_weight, value_weight, query_gain, key_gain, output_weight,
):
    n_sp, n_tp = lax.axis_size("sp"), lax.axis_size("tp")
    row_slab, columns = shift_weight.shape
    own_rows, model = latent.shape
    ctx_rows = context.shape[0]
    tok = own_rows * n_tp
    q_width, kv_width = query_weight.shape[1], key_weight.shape[1]
    groups = kv_width // SPAN
    heads = q_width // SPAN // groups
    chips = n_tp // 2
    width = 2 * own_rows
    lows = 2 ** (int(math.log2(n_sp)) // 2)
    highs = n_sp // lows
    slots = chips * n_sp + n_sp * ctx_rows // width
    n_tiles = chips * groups
    split = 2 if width // 2 % 128 == 0 else 1
    bands = columns // 128
    offset = math.log(tok / (2.0 * ctx_rows))
    dma = pltpu.SemaphoreType.DMA

    def stay(a):
        return pltpu.with_memory_space_constraint(a, pltpu.HBM)

    return pl.pallas_call(
        functools.partial(kernel, n_sp, n_tp, lows, offset, split),
        out_shape=jax.ShapeDtypeStruct(latent.shape, BF16),
        in_specs=[ANY] * 14,
        out_specs=VMEM,
        scratch_shapes=[
            pltpu.VMEM((1, model), F32), pltpu.VMEM((1, model), F32), pltpu.VMEM((1, model), F32),
            pltpu.VMEM((1, SPAN), F32), pltpu.VMEM((1, SPAN), F32),
            pltpu.VMEM((chips, width, model), BF16),
            pltpu.VMEM(context.shape, BF16),
            pltpu.VMEM((3, row_slab, columns), BF16),
            pltpu.VMEM((model, q_width + 2 * kv_width), BF16),
            pltpu.VMEM((2,) + (key_weight.shape if kv_width % 128 else (16, 128)), BF16),
            pltpu.VMEM(output_weight.shape, BF16),
            pltpu.VMEM((4 * bands, 128), F32),
            pltpu.VMEM((n_sp, 4 * bands, 128), F32),
            pltpu.VMEM((n_tp, 4 * bands, 128), F32),
            pltpu.VMEM((8, 128), F32),
            pltpu.VMEM((n_sp, 8, 128), F32),
            pltpu.VMEM((n_tp, 8, 128), F32),
            pltpu.VMEM((8, model), F32),
            pltpu.VMEM((width, model), BF16),
            pltpu.VMEM((chips, SPAN, width), F32),
            pltpu.VMEM((SPAN, width), F32),
            pltpu.VMEM((SPAN, width), F32),
            pltpu.VMEM((chips, groups, heads, SPAN, width), BF16),
            pltpu.VMEM((chips, groups, heads, SPAN, width), BF16),
            pltpu.VMEM((chips, groups, 2 * SPAN, width), BF16),
            pltpu.VMEM((groups, ctx_rows, 2 * SPAN), BF16),
            pltpu.VMEM((n_sp, ctx_rows, 2 * SPAN), BF16),
            pltpu.VMEM((n_tiles, heads, 2 * SPAN, width), BF16),
            pltpu.VMEM((slots, 2 * SPAN + 16, width), BF16),
            pltpu.VMEM((slots, width, 2 * SPAN), BF16),
            pltpu.VMEM((n_tiles, heads, 8, width), F32),
            pltpu.VMEM((n_tiles, heads, SPAN + 16, width), F32),
            pltpu.VMEM((chips, groups, width, 2 * SPAN), BF16),
            pltpu.VMEM((n_tp * groups, own_rows, 2 * SPAN), BF16),
            dma((9,)), dma((chips, PIECES)), dma((max(chips - 1, 1), PIECES)), dma((n_tp, PIECES)),
            dma((2, n_sp - 1)), dma((2, n_sp - 1)), dma((2, n_tp - 1)), dma((2, n_tp - 1)),
            dma((chips, split, max(groups - 1, 1))), dma((chips, split, groups)),
            dma((chips, split, highs - 1)), dma((chips, split, lows - 1)),
            dma((chips, split, highs - 1, lows - 1)), dma((chips, split, n_sp)),
            dma((highs - 1,)), dma((lows - 1,)), dma((highs - 1, lows - 1)), dma((n_sp,)),
            dma((chips, groups, 2)), dma((n_tp * groups,)), dma((5,)),
            pltpu.VMEM(latent.shape, F32), pltpu.VMEM((width, 128), F32),
        ],
        compiler_params=pltpu.CompilerParams(
            collective_id=0, has_side_effects=True, vmem_limit_bytes=46 << 20
        ),
        name="fused",
    )(
        stay(latent), stay(context), stay(condition[None]), stay(context_condition[None]),
        stay(norm_gain[None]),
        stay(shift_weight), stay(scale_weight), stay(gate_weight), stay(query_weight),
        stay(key_weight), stay(value_weight), stay(query_gain[None]), stay(key_gain[None]),
        stay(output_weight),
    )


def solution(mesh):
    in_specs = (
        P(("sp", "tp"), None), P("sp", None), P(), P(), P(),
        P("sp", "tp"), P("sp", "tp"), P("sp", "tp"),
        P(None, "tp"), P(None, "tp"), P(None, "tp"), P(), P(), P(),
    )
    return jax.shard_map(
        on_device, mesh=mesh, in_specs=in_specs, out_specs=P(("sp", "tp"), None), check_vma=False
    )
```

```python
import functools
import math

import jax
import jax.numpy as jnp
from jax import lax
from jax.experimental import pallas as pl
from jax.experimental.pallas import tpu as pltpu
from jax.sharding import PartitionSpec as P

SPAN = 64
GRID_W = 64
QUARTER = SPAN // 4
LAG = 5
OWE = 0
PIECES = 2
LOG2E = 1.4426950408889634
MESH = pl.DeviceIdType.MESH
VMEM = pl.BlockSpec(memory_space=pltpu.VMEM)
ANY = pl.BlockSpec(memory_space=pl.ANY)
F32 = jnp.float32
BF16 = jnp.bfloat16

epsilon = 1e-06
rope_base = 10000.0


def kernel(
    n_sp, n_tp, lows, offset, split,
    latent_hbm, context_hbm, cond_hbm, ctx_cond_hbm, norm_gain_hbm, w_shift_hbm, w_scale_hbm,
    w_gate_hbm, w_q_hbm, w_k_hbm, w_v_hbm, q_gain_hbm, k_gain_hbm, w_out_hbm,
    out, cond, ctx_cond, norm_gain, q_gain, k_gain,
    lat, context, w_mod, w_all, w_side, w_out, part, parts, mods, part_g, parts_g, mods_g,
    coef, hidden, table, gain_q, gain_k, q_send, q_raw, kv_send, ctx_send, ctx_all, q_all, kv_all,
    k_nat, peak, acc, attended, received,
    load, lat_send, lat_fwd, lat_recv, sp_send, sp_recv, tp_send, tp_recv,
    q_ssem, q_rsem, z_send, y_send, f_send, kv_recv,
    cz_send, cy_send, cf_send, c_recv, at_send, at_recv, small_sem, summed_out, inverse,
):
    sp, tp = lax.axis_index("sp"), lax.axis_index("tp")
    chips = n_tp // 2
    highs = n_sp // lows
    low, high = lax.rem(sp, lows), sp // lows
    x, core = tp // 2, lax.rem(tp, 2)
    twin = tp + 1 - 2 * core
    width = lat.shape[1]
    own_rows = width // 2
    model = lat.shape[2]
    tok = chips * width
    ctx_rows = context.shape[0]
    groups = kv_send.shape[1]
    heads = q_send.shape[2]
    q_width = groups * heads * SPAN
    kv_width = groups * SPAN
    row_slab, columns = w_mod.shape[1], w_mod.shape[2]
    bands = columns // 128
    g = lax.rem(high, groups)
    base = high - g
    ctx_slots = n_sp * ctx_rows // width
    ctx_first = chips * n_sp
    step = own_rows // PIECES
    part_width = width // split

    def dev(z, y):
        return z * lows + y

    def remote(src, dst, ssem, rsem, peer):
        return pltpu.make_async_remote_copy(
            src_ref=src, dst_ref=dst, send_sem=ssem, recv_sem=rsem,
            device_id=peer, device_id_type=MESH,
        )

    def lanes_of(d, p):
        if d == 0 or split == 1:
            return slice(0, width)
        return slice(p * part_width, (p + 1) * part_width)

    def parts_in(d):
        return 1 if d == 0 else split

    barrier = pltpu.get_barrier_semaphore()
    peers = [(lax.rem(sp + d, n_sp), tp) for d in range(1, n_sp)]
    peers += [(sp, lax.rem(tp + d, n_tp)) for d in range(1, n_tp)]
    for r in range(1, groups):
        mate = dev(base + lax.rem(g + r, groups), low)
        peers += [(mate, lax.rem(tp + d, n_tp)) for d in range(1, n_tp)]
    for p in peers:
        pl.semaphore_signal(barrier, inc=1, device_id=p, device_id_type=MESH)

    mine_rows = pl.ds(pl.multiple_of(core * own_rows, own_rows), own_rows)
    pairs = [
        (w_shift_hbm, w_mod.at[0]), (w_scale_hbm, w_mod.at[1]),
        (latent_hbm, lat.at[x, mine_rows, :]), (w_gate_hbm, w_mod.at[2]),
        (context_hbm, context), (w_q_hbm, w_all.at[:, 0:q_width]),
    ]
    if kv_width % 128 == 0:
        pairs += [
            (w_k_hbm, w_all.at[:, q_width : q_width + kv_width]),
            (w_v_hbm, w_all.at[:, q_width + kv_width :]),
        ]
    else:
        pairs += [(w_k_hbm, w_side.at[0]), (w_v_hbm, w_side.at[1])]
    pairs.append((w_out_hbm, w_out))
    small = [
        pltpu.make_async_copy(s, d, small_sem.at[i])
        for i, (s, d) in enumerate(
            (
                (cond_hbm, cond), (ctx_cond_hbm, ctx_cond), (norm_gain_hbm, norm_gain),
                (q_gain_hbm, q_gain), (k_gain_hbm, k_gain),
            )
        )
    ]
    for c in small:
        c.start()
    loads = [pltpu.make_async_copy(s, d, load.at[i]) for i, (s, d) in enumerate(pairs)]
    for c in loads[:-1]:
        c.start()

    def slab(ref):
        if row_slab % 128 == 0:
            return ref[:, pl.ds(pl.multiple_of(sp * row_slab, 128), row_slab)]
        per = 128 // row_slab
        window = ref[:, pl.ds(pl.multiple_of(sp // per * 128, 128), 128)]
        pick = lax.rem(sp, per)
        result = window
        for k in range(1, per):
            result = jnp.where(pick == k, pltpu.roll(window, 128 - k * row_slab, 1), result)
        return result[:, :row_slab]

    for c in small:
        c.wait()
    v = jnp.concatenate([slab(cond), slab(ctx_cond)], axis=0)
    act = (v / (1.0 + jnp.exp(-v))).astype(BF16)
    part_g[...] = jnp.zeros_like(part_g)
    for i in range(2):
        loads[i].wait()
        r = jnp.dot(act, w_mod[i], preferred_element_type=F32)
        for row in range(2):
            for k in range(bands):
                at = (2 * i + row) * bands + k
                part[at : at + 1, :] = r[row : row + 1, k * 128 : (k + 1) * 128]
    loads[2].wait()
    pl.semaphore_wait(barrier, len(peers))

    def rows_of(tile, piece):
        chip, half = tile // 2, lax.rem(tile, 2)
        start = pl.multiple_of(half * own_rows + piece * step, step)
        return lat.at[chip, pl.ds(start, step), :]

    def row_copy(tile, piece, ssem, peer):
        return remote(
            rows_of(tile, piece), rows_of(tile, piece), ssem, lat_recv.at[tile, piece], (sp, peer)
        )

    lat_sends = []

    def send_piece(piece):
        for d in range(1, chips):
            c = row_copy(tp, piece, lat_send.at[d, piece], lax.rem(tp + 2 * d, n_tp))
            c.start()
            lat_sends.append(c)

    sp_copies = []
    for d in range(1, n_sp):
        c = remote(
            part, parts.at[sp], sp_send.at[0, d - 1], sp_recv.at[0, d - 1],
            (lax.rem(sp + d, n_sp), tp),
        )
        c.start()
        sp_copies.append(c)
    send_piece(0)
    for piece in range(PIECES):
        c = row_copy(tp, piece, lat_send.at[0, piece], twin)
        c.start()
        lat_sends.append(c)
    parts[sp] = part[...]

    loads[3].wait()
    r = jnp.dot(act, w_mod[2], preferred_element_type=F32)
    for k in range(bands):
        part_g[k : k + 1, :] = r[0:1, k * 128 : (k + 1) * 128]
    parts_g[sp] = part_g[...]
    loads[-1].start()
    for d in range(chips):
        chip = lax.rem(x - d + chips, chips)
        lane = lax.broadcasted_iota(jnp.int32, (QUARTER, width), 1)
        if parts_in(d) > 1:
            lane = lane // step % 2 * own_rows + lane // part_width * step + lane % step
        place = sp * tok + chip * width + lane
        turn = lax.broadcasted_iota(jnp.int32, (QUARTER, width), 0).astype(F32)
        freq = jnp.exp(turn * (-math.log(rope_base) / QUARTER))
        by_row = (place // GRID_W).astype(F32) * freq
        by_col = (place % GRID_W).astype(F32) * freq
        table[d, 0:QUARTER, :] = jnp.cos(by_row)
        table[d, QUARTER : 2 * QUARTER, :] = jnp.sin(by_row)
        table[d, 2 * QUARTER : 3 * QUARTER, :] = jnp.cos(by_col)
        table[d, 3 * QUARTER :, :] = jnp.sin(by_col)
    k_pair = jnp.concatenate([k_gain[...], k_gain[...]], axis=1)
    for ref, dst in ((q_gain, gain_q), (k_gain, gain_k)):
        row = jnp.concatenate([ref[...], ref[...]], axis=1)
        square = jnp.transpose(jnp.broadcast_to(row, (128, 128)))[0:SPAN, :]
        for c in range(0, width, 128):
            dst[:, c : c + 128] = square
    peak[...] = jnp.full_like(peak, -1e30)
    acc[...] = jnp.zeros_like(acc)
    kv_all[:, 2 * SPAN :, :] = jnp.ones((kv_all.shape[0], 16, width), BF16)

    for c in sp_copies:
        c.wait()
    summed = parts[0]
    for j in range(1, n_sp):
        summed = summed + parts[j]
    part[...] = summed
    mods[tp] = summed
    tp_copies = []
    for d in range(1, n_tp):
        c = remote(
            part, mods.at[tp], tp_send.at[0, d - 1], tp_recv.at[0, d - 1],
            (sp, lax.rem(tp + d, n_tp)),
        )
        c.start()
        tp_copies.append(c)
    for piece in range(1, PIECES):
        send_piece(piece)
    gate_copies = []
    for d in range(1, n_sp):
        c = remote(
            part_g, parts_g.at[sp], sp_send.at[1, d - 1], sp_recv.at[1, d - 1],
            (lax.rem(sp + d, n_sp), tp),
        )
        c.start()
        gate_copies.append(c)
    for c in loads[4:-1]:
        c.wait()
    if kv_width % 128 != 0:
        w_all[:, q_width:] = jnp.concatenate([w_side[0], w_side[1]], axis=1)
    for piece in range(PIECES):
        row_copy(twin, piece, lat_send.at[0, 0], twin).wait_recv()

    def measure(i, carry):
        r = pl.ds(pl.multiple_of(i * 16, 16), 16)
        w = lat[x, r, :].astype(F32)
        inv = lax.rsqrt(jnp.sum(w * w, axis=-1, keepdims=True) / model + epsilon)
        inverse[r, :] = jnp.broadcast_to(inv, (16, 128))
        return carry

    lax.fori_loop(0, width // 16, measure, 0, unroll=4)
    for c in tp_copies:
        c.wait()
    for t in range(n_tp):
        for k in range(bands):
            cols = slice(t * columns + k * 128, t * columns + (k + 1) * 128)
            for row in range(2):
                at = (2 + row) * bands + k
                coef[row : row + 1, cols] = norm_gain[:, cols] * (1.0 + mods[t, at : at + 1, :])
                at = row * bands + k
                coef[2 + row : 3 + row, cols] = mods[t, at : at + 1, :]

    block = 16

    def modulate(read, rows, first, row, known=False):
        def body(i, carry):
            w = read(i * block).astype(F32)
            if known:
                r = pl.ds(pl.multiple_of(i * block, block), block)
                inv = jnp.concatenate([inverse[r, :]] * (model // 128), axis=1)
            else:
                inv = lax.rsqrt(jnp.sum(w * w, axis=-1, keepdims=True) / model + epsilon)
            y = w * inv * coef[row : row + 1, :] + coef[2 + row : 3 + row, :]
            hidden[pl.ds(pl.multiple_of(first + i * block, block), block), :] = y.astype(BF16)
            return carry

        lax.fori_loop(0, rows // block, body, 0, unroll=min(4, rows // block))

    z_order = [d for d in range(1, highs)]
    z_order = z_order[1:2] + z_order[:1] + z_order[2:]
    tail_sends = []

    def begin(c):
        c.start()
        tail_sends.append(c)

    def ctx_copy(head, src, ssem, z, y):
        return remote(ctx_send.at[head], ctx_all.at[src], ssem, c_recv.at[src], (dev(z, y), tp))

    def context_step():
        modulate(
            lambda i: context[pl.ds(pl.multiple_of(i, block), block), :], ctx_rows, 0, 1
        )
        raw = jnp.dot(hidden[0:ctx_rows, :], w_all[:, q_width:], preferred_element_type=F32)
        if groups == 2:
            k, val = raw[:, :kv_width], raw[:, kv_width:]
            first = lax.broadcasted_iota(jnp.int32, k.shape, 1) < SPAN
            sq = k * k
            s0 = jnp.sum(jnp.where(first, sq, 0.0), axis=-1, keepdims=True)
            s1 = jnp.sum(jnp.where(first, 0.0, sq), axis=-1, keepdims=True)
            scale = jnp.where(
                first, lax.rsqrt(s0 / SPAN + epsilon), lax.rsqrt(s1 / SPAN + epsilon)
            )
            k = k * scale * k_pair
            ctx_send[0] = jnp.where(first, k, pltpu.roll(val, SPAN, 1)).astype(BF16)
            ctx_send[1] = jnp.where(first, pltpu.roll(k, SPAN, 1), val).astype(BF16)
        else:
            first = lax.broadcasted_iota(jnp.int32, raw.shape, 1) < SPAN
            s0 = jnp.sum(jnp.where(first, raw * raw, 0.0), axis=-1, keepdims=True)
            k = raw * lax.rsqrt(s0 / SPAN + epsilon) * k_pair
            ctx_send[0] = jnp.where(first, k, raw).astype(BF16)
        for dz in z_order:
            z = lax.rem(high + dz, highs)
            begin(ctx_copy(lax.rem(z, groups), sp, cz_send.at[dz - 1], z, low))
        for dl in range(1, lows):
            begin(ctx_copy(g, sp, cy_send.at[dl - 1], high, lax.rem(low + dl, lows)))
        ctx_all[sp] = ctx_send[g]

    def finish(raw_head, gain, d, lanes):
        n = lanes.stop - lanes.start
        inv = lax.rsqrt(jnp.sum(raw_head * raw_head, axis=0, keepdims=True) / SPAN + epsilon)
        y = raw_head * inv * gain[:, 0:n]
        a1, b1 = y[0:QUARTER], y[QUARTER : 2 * QUARTER]
        a2, b2 = y[2 * QUARTER : 3 * QUARTER], y[3 * QUARTER :]
        cr, sr = table[d, 0:QUARTER, lanes], table[d, QUARTER : 2 * QUARTER, lanes]
        cc, sc = table[d, 2 * QUARTER : 3 * QUARTER, lanes], table[d, 3 * QUARTER :, lanes]
        return jnp.concatenate(
            [a1 * cr - b1 * sr, b1 * cr + a1 * sr, a2 * cc - b2 * sc, b2 * cc + a2 * sc], axis=0
        )

    def q_copy(d, p, group, ssem, z):
        lanes = lanes_of(d, p)
        return remote(
            q_send.at[d, group, :, :, lanes], q_raw.at[d, g, :, :, lanes], ssem,
            q_rsem.at[d, p, g], (dev(z, low), tp),
        )

    def q_store(d, group, value):
        f = value.astype(F32) * LOG2E
        hi = f.astype(BF16)
        q_all[d * groups + group, :, 0:SPAN, :] = hi
        q_all[d * groups + group, :, SPAN:, :] = (f - hi.astype(F32)).astype(BF16)

    def q_own(d):
        q_store(d, g, q_send[d, g])

    def q_arrive(d):
        for r in range(1, groups):
            other = lax.rem(g + r, groups)
            for p in range(parts_in(d)):
                lanes = lanes_of(d, p)
                dst = q_raw.at[d, other, :, :, lanes]
                remote(
                    dst, dst, q_ssem.at[d, 0, 0], q_rsem.at[d, p, other], (dev(base + other, low), tp)
                ).wait_recv()
            q_store(d, other, q_raw[d, other])

    def kv_copy(src_ref, d, p, src, ssem, z, y):
        lanes = lanes_of(d, p)
        return remote(
            src_ref, kv_all.at[d * n_sp + src, 0 : 2 * SPAN, lanes], ssem, kv_recv.at[d, p, src],
            (dev(z, y), tp),
        )

    def key_rows(slot, lanes):
        k = kv_all[slot, 0:SPAN, lanes]
        k_nat[slot, lanes, :] = jnp.transpose(jnp.concatenate([k, k], axis=0))

    def project(d, p):
        chip = lax.rem(x - d + chips, chips)
        lanes = lanes_of(d, p)
        n = lanes.stop - lanes.start
        if n == width:
            modulate(
                lambda i: lat[chip, pl.ds(pl.multiple_of(i, block), block), :], width, 0, 0, d == 0
            )
        else:
            for half in range(2):
                at = half * own_rows + p * step
                modulate(
                    lambda i: lat[chip, pl.ds(pl.multiple_of(at + i, block), block), :],
                    step, half * step, 0,
                )
        flat = jnp.dot(hidden[0:n, :], w_all[...], preferred_element_type=F32)
        up = jnp.transpose(flat)
        for j in range(groups):
            r = q_width + j * SPAN
            kv_send[d, j, 0:SPAN, lanes] = finish(up[r : r + SPAN], gain_k, d, lanes).astype(BF16)
            r = q_width + kv_width + j * SPAN
            kv_send[d, j, SPAN:, lanes] = up[r : r + SPAN].astype(BF16)
            for h in range(heads):
                r = (j * heads + h) * SPAN
                y = finish(up[r : r + SPAN], gain_q, d, lanes)
                q_send[d, j, h, :, lanes] = (y * SPAN ** (-0.5)).astype(BF16)
        if d == 0:
            for r in range(1, groups):
                other = lax.rem(g + r, groups)
                begin(q_copy(d, p, other, q_ssem.at[d, p, r - 1], base + other))
        for dz in z_order:
            z = lax.rem(high + dz, highs)
            src = kv_send.at[d, lax.rem(z, groups), :, lanes]
            begin(kv_copy(src, d, p, sp, z_send.at[d, p, dz - 1], z, low))
        for dl in range(1, lows):
            y = lax.rem(low + dl, lows)
            src = kv_send.at[d, g, :, lanes]
            begin(kv_copy(src, d, p, sp, y_send.at[d, p, dl - 1], high, y))
        if d > 0:
            for r in range(1, groups):
                other = lax.rem(g + r, groups)
                begin(q_copy(d, p, other, q_ssem.at[d, p, r - 1], base + other))
        kv_all[d * n_sp + sp, 0 : 2 * SPAN, lanes] = kv_send[d, g, :, lanes]
        key_rows(d * n_sp + sp, lanes)

    def column(d, p, dz):
        src = dev(lax.rem(high - dz + highs, highs), low)
        slot = d * n_sp + src
        lanes = lanes_of(d, p)
        here = kv_all.at[slot, 0 : 2 * SPAN, lanes]
        kv_copy(here, d, p, src, z_send.at[0, 0, 0], high, low).wait_recv()
        for dl in range(1, lows):
            y = lax.rem(low + dl, lows)
            begin(kv_copy(here, d, p, src, f_send.at[d, p, dz - 1, dl - 1], high, y))
        key_rows(slot, lanes)

    def ctx_column(dz):
        src = dev(lax.rem(high - dz + highs, highs), low)
        ctx_copy(0, src, cz_send.at[0], high, low).wait_recv()
        for dl in range(1, lows):
            y = lax.rem(low + dl, lows)
            begin(
                remote(
                    ctx_all.at[src], ctx_all.at[src], cf_send.at[dz - 1, dl - 1],
                    c_recv.at[src], (dev(high, y), tp),
                )
            )

    def side(d, dz, dl):
        src = dev(lax.rem(high - dz + highs, highs), lax.rem(low - dl + lows, lows))
        slot = d * n_sp + src
        for p in range(parts_in(d)):
            lanes = lanes_of(d, p)
            here = kv_all.at[slot, 0 : 2 * SPAN, lanes]
            kv_copy(here, d, p, src, z_send.at[0, 0, 0], high, low).wait_recv()
            key_rows(slot, lanes)

    def ctx_ready():
        for dl in range(1, lows):
            for dz in range(highs):
                src = dev(lax.rem(high - dz + highs, highs), lax.rem(low - dl + lows, lows))
                ctx_copy(0, src, cz_send.at[0], high, low).wait_recv()
        per = width // ctx_rows
        for c in range(ctx_slots):
            piece = ctx_all[c * per : (c + 1) * per].reshape(width, 2 * SPAN)
            kv_all[ctx_first + c, 0 : 2 * SPAN, :] = jnp.transpose(piece)
            key_rows(ctx_first + c, slice(0, width))

    def slot_of(d, dz, dl):
        return d * n_sp + dev(
            lax.rem(high - dz + highs, highs), lax.rem(low - dl + lows, lows)
        )

    def run(steps):
        queue, owed = [], []

        def settle(limit):
            while len(owed) > limit:
                w, shrink, t, h, action = owed.pop(0)
                acc[t, h] = acc[t, h] * shrink + w
                if action is not None:
                    settle(0)
                    action()

        def soft():
            s, slot, t, h, action = queue.pop(0)
            old = peak[t, h, 0:1, :]
            top = jnp.maximum(jnp.max(s, axis=0, keepdims=True), old)
            shrink = jnp.exp2(old - top)
            e = jnp.exp2(s - top).astype(BF16)
            peak[t, h] = jnp.broadcast_to(top, (8, width))
            w = jnp.dot(kv_all[slot, SPAN:, :], e, preferred_element_type=F32)
            owed.append((w, shrink, t, h, action))
            settle(OWE)

        for kind, *rest in steps:
            if kind == "do":
                rest[0]()
                continue
            slot, t, action = rest
            for h in range(heads):
                r = jnp.dot(k_nat[slot], q_all[t, h], preferred_element_type=F32)
                if isinstance(slot, int) and slot >= ctx_first:
                    r = r + offset * LOG2E
                queue.append((r, slot, t, h, action if h == heads - 1 else None))
                if len(queue) > LAG:
                    soft()
        while queue:
            soft()
        settle(0)

    def attend(items):
        run([("at", s, t, None) for s, t in items])

    def attend_range(first, count, tile_list):
        per = math.gcd(max(1, 8 // len(tile_list)), count)

        def body(i, carry):
            attend([(first + i * per + u, t) for u in range(per) for t in tile_list])
            return carry

        lax.fori_loop(0, count // per, body, 0)

    def fetch(d, piece):
        chip = lax.rem(x - d + chips, chips)
        near = 2 * chip + core
        row_copy(near, piece, lat_send.at[0, 0], twin).wait_recv()
        begin(row_copy(near, piece, lat_fwd.at[d - 1, piece], twin))

    def fetch_back(d, piece):
        chip = lax.rem(x - d + chips, chips)
        row_copy(2 * chip + 1 - core, piece, lat_send.at[0, 0], twin).wait_recv()

    copies = []

    def deliver(d, r):
        chip = lax.rem(x - d + chips, chips)
        j = lax.rem(g + r, groups)
        t = d * groups + j
        rows = []
        for h in range(heads):
            inv = 1.0 / acc[t, h, SPAN : SPAN + 1, :]
            rows.append(acc[t, h, 0:SPAN, :] * inv)
        turned = jnp.transpose(jnp.concatenate(rows, axis=0)).astype(BF16)
        if parts_in(d) == 1:
            attended[d, r] = turned
        else:
            for p in range(split):
                for half in range(2):
                    at = half * own_rows + p * step
                    took = p * part_width + half * step
                    attended[d, r, at : at + step, :] = turned[took : took + step]
        for rc in range(2):
            half = lax.rem(core + rc, 2)
            src = attended.at[d, r, pl.ds(pl.multiple_of(half * own_rows, own_rows), own_rows), :]
            if d == 0 and r == 0 and rc == 0:
                received[tp * groups + g] = src[...]
            else:
                c = remote(
                    src, received.at[tp * groups + g], at_send.at[d, r, rc],
                    at_recv.at[tp * groups + g], (dev(base + j, low), 2 * chip + half),
                )
                c.start()
                copies.append(c)

    def gates():
        for c in gate_copies:
            c.wait()
        whole = parts_g[0]
        for j in range(1, n_sp):
            whole = whole + parts_g[j]
        part_g[...] = whole
        mods_g[tp] = whole
        result = []
        for d in range(1, n_tp):
            c = remote(
                part_g, mods_g.at[tp], tp_send.at[1, d - 1], tp_recv.at[1, d - 1],
                (sp, lax.rem(tp + d, n_tp)),
            )
            c.start()
            result.append(c)
        return result

    def tile_of(d, r):
        return d * groups + lax.rem(g + r, groups)

    if chips == 2 and split == 2 and n_sp == 8 and groups == 2:
        project(0, 0)
        fetch(1, 0)
        context_step()
        fetch_back(1, 0)
        project(1, 0)
        gate_out = gates()
        za, zb, zc = z_order
        own_a, mate_a, own_b, mate_b = (tile_of(d, r) for d in range(2) for r in range(2))
        early = [own_a, mate_a]
        ctx = range(ctx_first, ctx_first + ctx_slots)
        steps = []

        def do(action, *given):
            steps.append(("do", functools.partial(action, *given)))

        def at(slots, tiles):
            steps.extend(("at", s, t, None) for s in slots for t in tiles)

        q_own(0)
        q_arrive(0)
        at([slot_of(0, 0, 0)], early)
        do(side, 0, 0, 1)
        at([slot_of(0, 0, 1)], early)
        do(column, 0, 0, za)
        do(fetch, 1, 1)
        at([slot_of(0, za, 0)], early)
        do(column, 0, 0, zb)
        at([slot_of(0, zb, 0)], early)
        do(fetch_back, 1, 1)
        do(project, 1, 1)
        do(q_own, 1)
        do(column, 0, 0, zc)
        most = early + [own_b]
        at([slot_of(0, zc, 0), slot_of(1, 0, 0)], most)
        at([slot_of(0, dz, 0) for dz in (0, za, zb)] + [slot_of(0, 0, 1)], [own_b])
        for dz in z_order:
            do(ctx_column, dz)
        do(column, 1, 0, za)
        do(side, 0, za, 1)
        at([slot_of(0, za, 1)], most)
        do(column, 1, 0, zb)
        do(side, 0, zb, 1)
        at([slot_of(0, zb, 1)], most)
        do(column, 1, 0, zc)
        do(side, 0, zc, 1)
        at([slot_of(0, zc, 1)], most)
        do(ctx_ready)
        at(ctx, most)
        do(side, 1, 0, 1)
        at([slot_of(1, 0, 1)], most)
        do(column, 1, 1, za)
        at([slot_of(1, za, 0)], most)
        do(column, 1, 1, zb)
        at([slot_of(1, zb, 0)], most)
        do(column, 1, 1, zc)
        do(q_arrive, 1)
        at(range(n_sp), [mate_b])
        at(ctx, [mate_b])
        at([slot_of(1, zc, 0)], most)
        at([slot_of(1, dz, 0) for dz in [0] + z_order] + [slot_of(1, 0, 1)], [mate_b])
        every = [mate_a, mate_b, own_b, own_a]
        do(side, 1, za, 1)
        at([slot_of(1, za, 1)], every)
        do(side, 1, zb, 1)
        do(side, 1, zc, 1)
        for place, t in zip(((0, 1), (1, 1), (1, 0), (0, 0)), every):
            at([slot_of(1, zb, 1)], [t])
            end = functools.partial(deliver, *place)
            steps.append(("at", slot_of(1, zc, 1), t, end))
        run(steps)
    else:
        context_step()
        for d in range(chips):
            if d > 0:
                for piece in range(PIECES):
                    fetch(d, piece)
                for piece in range(PIECES):
                    fetch_back(d, piece)
            for p in range(parts_in(d)):
                project(d, p)
            q_own(d)
        gate_out = gates()
        for dz in z_order:
            ctx_column(dz)
        for d in range(chips):
            for p in range(parts_in(d)):
                for dz in z_order:
                    column(d, p, dz)
            q_arrive(d)
        ctx_ready()
        for d in range(chips):
            for dl in range(1, lows):
                for dz in range(highs):
                    side(d, dz, dl)
        for d in range(chips):
            for r in range(groups):
                t = tile_of(d, r)
                attend_range(0, ctx_first, [t])
                attend([(s, t) for s in range(ctx_first, ctx_first + ctx_slots)])
                deliver(d, r)

    loads[-1].wait()
    for c in gate_out:
        c.wait()
    order = [tp, twin]
    for d in range(1, chips):
        order += [lax.rem(tp + 2 * d, n_tp), lax.rem(twin + 2 * d, n_tp)]
    for n, src in enumerate(order):
        for r in range(groups):
            if n == 0 and r == 0:
                continue
            who = src * groups + lax.rem(g + r, groups)
            remote(
                received.at[who], received.at[who], at_send.at[0, 0, 1], at_recv.at[who],
                (sp, twin),
            ).wait_recv()
        depth = groups * 2 * SPAN
        rows = jnp.concatenate([received[src * groups + j] for j in range(groups)], axis=1)
        heights = pl.ds(pl.multiple_of(src * depth, depth), depth)
        for t in range(n_tp):
            cols = slice(t * columns, (t + 1) * columns)
            branch = jnp.dot(rows, w_out[heights, cols], preferred_element_type=F32)
            if n > 0:
                branch = branch + summed_out[:, cols]
            if n < len(order) - 1:
                summed_out[:, cols] = branch
            else:
                gate = jnp.concatenate([mods_g[t, k : k + 1, :] for k in range(bands)], axis=1)
                out[:, cols] = (lat[x, mine_rows, cols].astype(F32) + gate * branch).astype(BF16)
    for c in lat_sends + tail_sends + copies:
        c.wait_send()


def on_device(
    latent, context, condition, context_condition, norm_gain, shift_weight, scale_weight,
    gate_weight, query_weight, key_weight, value_weight, query_gain, key_gain, output_weight,
):
    n_sp, n_tp = lax.axis_size("sp"), lax.axis_size("tp")
    row_slab, columns = shift_weight.shape
    own_rows, model = latent.shape
    ctx_rows = context.shape[0]
    tok = own_rows * n_tp
    q_width, kv_width = query_weight.shape[1], key_weight.shape[1]
    groups = kv_width // SPAN
    heads = q_width // SPAN // groups
    chips = n_tp // 2
    width = 2 * own_rows
    lows = 2 ** (int(math.log2(n_sp)) // 2)
    highs = n_sp // lows
    slots = chips * n_sp + n_sp * ctx_rows // width
    n_tiles = chips * groups
    split = 2 if width // 2 % 128 == 0 else 1
    bands = columns // 128
    offset = math.log(tok / (2.0 * ctx_rows))
    dma = pltpu.SemaphoreType.DMA

    def stay(a):
        return pltpu.with_memory_space_constraint(a, pltpu.HBM)

    return pl.pallas_call(
        functools.partial(kernel, n_sp, n_tp, lows, offset, split),
        out_shape=jax.ShapeDtypeStruct(latent.shape, BF16),
        in_specs=[ANY] * 14,
        out_specs=VMEM,
        scratch_shapes=[
            pltpu.VMEM((1, model), F32), pltpu.VMEM((1, model), F32), pltpu.VMEM((1, model), F32),
            pltpu.VMEM((1, SPAN), F32), pltpu.VMEM((1, SPAN), F32),
            pltpu.VMEM((chips, width, model), BF16),
            pltpu.VMEM(context.shape, BF16),
            pltpu.VMEM((3, row_slab, columns), BF16),
            pltpu.VMEM((model, q_width + 2 * kv_width), BF16),
            pltpu.VMEM((2,) + (key_weight.shape if kv_width % 128 else (16, 128)), BF16),
            pltpu.VMEM(output_weight.shape, BF16),
            pltpu.VMEM((4 * bands, 128), F32),
            pltpu.VMEM((n_sp, 4 * bands, 128), F32),
            pltpu.VMEM((n_tp, 4 * bands, 128), F32),
            pltpu.VMEM((8, 128), F32),
            pltpu.VMEM((n_sp, 8, 128), F32),
            pltpu.VMEM((n_tp, 8, 128), F32),
            pltpu.VMEM((8, model), F32),
            pltpu.VMEM((width, model), BF16),
            pltpu.VMEM((chips, SPAN, width), F32),
            pltpu.VMEM((SPAN, width), F32),
            pltpu.VMEM((SPAN, width), F32),
            pltpu.VMEM((chips, groups, heads, SPAN, width), BF16),
            pltpu.VMEM((chips, groups, heads, SPAN, width), BF16),
            pltpu.VMEM((chips, groups, 2 * SPAN, width), BF16),
            pltpu.VMEM((groups, ctx_rows, 2 * SPAN), BF16),
            pltpu.VMEM((n_sp, ctx_rows, 2 * SPAN), BF16),
            pltpu.VMEM((n_tiles, heads, 2 * SPAN, width), BF16),
            pltpu.VMEM((slots, 2 * SPAN + 16, width), BF16),
            pltpu.VMEM((slots, width, 2 * SPAN), BF16),
            pltpu.VMEM((n_tiles, heads, 8, width), F32),
            pltpu.VMEM((n_tiles, heads, SPAN + 16, width), F32),
            pltpu.VMEM((chips, groups, width, 2 * SPAN), BF16),
            pltpu.VMEM((n_tp * groups, own_rows, 2 * SPAN), BF16),
            dma((9,)), dma((chips, PIECES)), dma((max(chips - 1, 1), PIECES)), dma((n_tp, PIECES)),
            dma((2, n_sp - 1)), dma((2, n_sp - 1)), dma((2, n_tp - 1)), dma((2, n_tp - 1)),
            dma((chips, split, max(groups - 1, 1))), dma((chips, split, groups)),
            dma((chips, split, highs - 1)), dma((chips, split, lows - 1)),
            dma((chips, split, highs - 1, lows - 1)), dma((chips, split, n_sp)),
            dma((highs - 1,)), dma((lows - 1,)), dma((highs - 1, lows - 1)), dma((n_sp,)),
            dma((chips, groups, 2)), dma((n_tp * groups,)), dma((5,)),
            pltpu.VMEM(latent.shape, F32), pltpu.VMEM((width, 128), F32),
        ],
        compiler_params=pltpu.CompilerParams(
            collective_id=0, has_side_effects=True, vmem_limit_bytes=46 << 20
        ),
        name="fused",
    )(
        stay(latent), stay(context), stay(condition[None]), stay(context_condition[None]),
        stay(norm_gain[None]),
        stay(shift_weight), stay(scale_weight), stay(gate_weight), stay(query_weight),
        stay(key_weight), stay(value_weight), stay(query_gain[None]), stay(key_gain[None]),
        stay(output_weight),
    )


def solution(mesh):
    in_specs = (
        P(("sp", "tp"), None), P("sp", None), P(), P(), P(),
        P("sp", "tp"), P("sp", "tp"), P("sp", "tp"),
        P(None, "tp"), P(None, "tp"), P(None, "tp"), P(), P(), P(),
    )
    return jax.shard_map(
        on_device, mesh=mesh, in_specs=in_specs, out_specs=P(("sp", "tp"), None), check_vma=False
    )
```
